32 devices in a mesh: sp: 8 (over z, y), tp: 4 (over x, core).
Axes of the slice: x: 2, y: 2, z: 4, core: 2. Of those that a mesh axis runs over, the one named last changes fastest.
Arguments:
- stream: bfloat16 [2048, 2048], P('sp', 'tp'), may hold values from -1200 to 1200, as said below
- mix_gain: bfloat16 [2048], P('tp'), may hold values from 0.099609375 to 1.8984375
- pool_weight: bfloat16 [4, 512, 512], P('tp'), may hold values from -0.25 to 0.25
- pool_scale: bfloat16 [2048], P('tp'), may hold values from 0.099609375 to 1.8984375
- ffn_gain: bfloat16 [2048], replicated, may hold values from 0.099609375 to 1.8984375
- routes: int32 [2048, 2], P(('sp', 'tp')), may hold values from 0 to 7, all different within a row; in each aligned block of 64 rows (0 to 63, 64 to 127, ...) at most 32 rows name the same one
- route_weight: float32 [2048, 2], P(('sp', 'tp')), may hold values from 0.1 to 1
- w_gate: bfloat16 [8, 2048, 7168], P('sp', None, 'tp'), may hold values from -0.125 to 0.125
- w_up: bfloat16 [8, 2048, 7168], P('sp', None, 'tp'), may hold values from -0.125 to 0.125
- w_down: bfloat16 [8, 7168, 2048], P('sp', 'tp'), may hold values from -0.0625 to 0.0625
Outputs:
- layer_out: bfloat16 [2048, 2048], P(('sp', 'tp'))
The draws below stay inside these ranges and needn't reach their ends.
Inputs may be any that keep to these rules, and one draw needn't show every extreme that they name: `routes`: each row names 2 different experts. Within each aligned block of 64 rows (the rows of one device) no expert is named by more than 32 rows, a bound that some block reaches. `stream`: finite values.
All inputs are finite; a program needn't handle non-finite values.
Results may differ from the reference program's by a relative error of at most 0.0061.
Values may be sent and summed in bfloat16 or wider, within the bound.
A program may use at most 128 MiB of HBM per device.

```python
import math
import jax
import jax.numpy as jnp
import numpy as np
from jax import lax

D = 2048
GROUPS = 4
FF = 7168
TOP = 2
GROUP_W = 512
TQ = 64
EXPERTS = 8
CAP = 32
TOKENS = 2048
N_SP = 8
N_TP = 4


def draw_stream(key, part):
    key_base = jax.random.fold_in(key, 11)
    key_cols = jax.random.fold_in(key, 12)
    base_draw = jnp.clip(jax.random.normal(key_base, (TOKENS, D), jnp.float32), -6.0, 6.0)
    col_scale = jnp.exp(jax.random.uniform(key_cols, (D,), jnp.float32) * math.log(10.0))
    group_index = (jnp.arange(D) // (D // GROUPS)).astype(jnp.float32)
    rise = 3.0 ** (group_index / (GROUPS - 1))
    values = base_draw / 8.0
    return (values * col_scale * rise).astype(jnp.bfloat16)


def block_scale(rng, extent, split, least, top_value):
    level = 1.0
    for dim, blocks in split:
        heights = jax.random.uniform(jax.random.fold_in(jax.random.fold_in(rng, 6), dim), (blocks,), jnp.float32, least / len(split), top_value / len(split))
        level = level * jnp.repeat(jnp.exp(heights), extent[dim] // blocks).reshape((-1,) + (1,) * (len(extent) - 1 - dim))
    return level


def deal_out(stream_key, own, number, rows, amount, top, bound, slope):
    ranking = jax.random.permutation(stream_key, amount)
    heavy_load, usual = portions_of(amount, rows * top, bound, slope, True), portions_of(amount, rows * top, bound, slope, False)
    places = jnp.arange(amount)

    def named(sizes, turn):
        used = int((sizes > 0).sum())
        fixed = max(1, used // 4)
        passed = fixed + (places - fixed + turn * (used - fixed)) % max(1, amount - fixed)
        return jnp.zeros((amount,), jnp.int32).at[ranking[jnp.where(places < fixed, places, passed)]].set(jnp.asarray(sizes, jnp.int32))

    sizes = jnp.where(number % 4 == 0, named(heavy_load, number // 4), named(usual, number - number // 4 - 1))
    mixed = jax.random.permutation(jax.random.fold_in(own, 3), amount)
    donor, receiver = mixed[0:amount // 2 * 2:2], mixed[1:amount // 2 * 2:2]
    slack = jnp.minimum(sizes[donor] - 1, bound - sizes[receiver]) // 2
    slack = jnp.where((donor == ranking[0]) | (receiver == ranking[0]) | (sizes[receiver] == 0), 0, jnp.maximum(slack, 0))
    passed = jax.random.randint(jax.random.fold_in(own, 4), (amount // 2,), 0, 1 << 20) % (slack + 1)
    sizes = sizes.at[donor].add(-passed).at[receiver].add(passed)
    members = jnp.searchsorted(jnp.cumsum(sizes), jnp.arange(rows * top), side="right").astype(jnp.int32)
    table = members.reshape(top, rows).T
    table = table[jax.random.permutation(jax.random.fold_in(own, 1), rows)]
    turn = jax.random.randint(jax.random.fold_in(own, 2), (rows, 1), 0, top)
    return jnp.take_along_axis(table, (jnp.arange(top)[None, :] + turn) % top, axis=1)


def portions_of(amount, total, bound, skew, full):
    portions = [(1 << 20) // math.isqrt(rank ** skew) + 1 for rank in range(1, amount + 1)]
    largest = bound if full else min(bound, max(-(-total // amount), total * portions[0] // sum(portions)))
    least = 1 if total - largest >= amount - 1 else 0
    given, rest = [largest] + [least] * (amount - 1), total - largest - least * (amount - 1)
    while rest > 0:
        free = [i for i in range(1, amount) if given[i] < largest] or [i for i in range(1, amount) if given[i] < bound]
        mass, left = sum([portions[i] for i in free]), rest
        for i in free:
            extra = min(bound - given[i], max(1, left * portions[i] // mass), rest)
            given[i] = given[i] + extra
            rest = rest - extra
    return np.array(given)


def gaussian(key, extent, spread, bound, shards=(), held_as=jnp.bfloat16):
    drawn = jax.random.normal(key, extent, jnp.float32) * spread
    if len(shards) > 0:
        drawn = block_scale(key, extent, shards, -0.22, 0.18) * drawn
    return jnp.clip(drawn, min=-bound, max=bound).astype(held_as)


def setup_inputs(seed: int = 0) -> dict:
    seeds = jax.random.split(jax.random.key(seed), 11)
    stream = draw_stream(jax.random.fold_in(seeds[10], 71), 0)
    mix_gain = jnp.clip(1.0 + 0.18 * jax.random.normal(seeds[1], (D,), jnp.float32), 0.099609375, 1.8984375).astype(jnp.bfloat16)
    pool_weight = gaussian(seeds[2], (GROUPS, GROUP_W, GROUP_W), GROUP_W ** -0.5, 0.25, ((0, 4),))
    pool_scale = jnp.clip(1.0 + 0.18 * jax.random.normal(seeds[3], (D,), jnp.float32), 0.099609375, 1.8984375).astype(jnp.bfloat16)
    ffn_gain = jnp.clip(1.0 + 0.18 * jax.random.normal(seeds[4], (D,), jnp.float32), 0.099609375, 1.8984375).astype(jnp.bfloat16)
    routes_keys = jax.random.split(jax.random.fold_in(seeds[5], 1), TOKENS // TQ)
    routes_turns = jax.random.permutation(jax.random.fold_in(seeds[5], 3), TOKENS // TQ)
    routes = jax.vmap(lambda own, number: deal_out(jax.random.fold_in(seeds[5], 2), own, number, TQ, EXPERTS, TOP, CAP, 1))(routes_keys, routes_turns).reshape((TOKENS, TOP))
    route_weight = jnp.clip(0.1 + 0.9 * jax.random.uniform(seeds[6], (TOKENS, TOP), jnp.float32) ** block_scale(seeds[6], (TOKENS, TOP), ((0, 32),), -0.2, 0.2), 0.1, 1.0)
    w_gate = gaussian(seeds[7], (EXPERTS, D, FF), D ** -0.5, 0.125, ((0, 8), (2, 4)))
    w_up = gaussian(seeds[8], (EXPERTS, D, FF), D ** -0.5, 0.125, ((0, 8), (2, 4)))
    w_down = gaussian(seeds[9], (EXPERTS, FF, D), FF ** -0.5, 0.0625, ((0, 8), (1, 4)))
    return dict(stream=stream, mix_gain=mix_gain, pool_weight=pool_weight, pool_scale=pool_scale, ffn_gain=ffn_gain, routes=routes, route_weight=route_weight, w_gate=w_gate, w_up=w_up, w_down=w_down)


NORM_EPS = 1e-06

def rms_norm(values, gain):
    row_scale = lax.rsqrt(lax.optimization_barrier(jnp.mean(values * values, axis=-1, keepdims=True)) + NORM_EPS)
    return (values * row_scale * gain.astype(jnp.float32)).astype(jnp.bfloat16)

def reference(stream, mix_gain, pool_weight, pool_scale, ffn_gain, routes, route_weight, w_gate, w_up, w_down):
    stream_f32 = stream.astype(jnp.float32)
    normed = rms_norm(stream_f32, mix_gain)
    normed_f32 = normed.astype(jnp.float32)
    group_width = D // GROUPS
    position = jnp.arange(1, TOKENS + 1).astype(jnp.float32)[:, None]
    group_outs = []
    for group_index in range(GROUPS):
        window_len = 2 ** (group_index + 1)
        columns = normed_f32[:, group_index * group_width:(group_index + 1) * group_width]
        window_sum = jnp.zeros_like(columns)
        for lag_rows in range(window_len):
            shifted = jnp.concatenate([jnp.zeros((lag_rows, group_width), jnp.float32), columns[:TOKENS - lag_rows]], axis=0)
            window_sum = window_sum + shifted
        pooled = (window_sum / jnp.minimum(position, jnp.float32(window_len)) - columns).astype(jnp.bfloat16)
        group_outs.append(jnp.dot(pooled, pool_weight[group_index], preferred_element_type=jnp.float32))
    mixer_out = jnp.concatenate(group_outs, axis=1) * pool_scale.astype(jnp.float32)
    after_mix = (stream_f32 + mixer_out).astype(jnp.bfloat16)
    after_f32 = after_mix.astype(jnp.float32)
    normed2 = rms_norm(after_f32, ffn_gain)
    flat_routes = routes.reshape(-1)
    flat_weight = route_weight.reshape(-1)
    max_rows = N_SP * N_TP * CAP
    ff_shard = FF // N_TP

    def one_expert(layer_sum, expert):
        chosen = flat_routes == expert
        picked = jnp.nonzero(chosen, size=max_rows, fill_value=0)[0].astype(jnp.int32)
        is_valid = (jnp.arange(max_rows) < jnp.sum(chosen.astype(jnp.int32))).astype(jnp.float32)
        token_index = picked // TOP
        expert_rows = normed2[token_index]
        gate_val = jnp.dot(expert_rows, w_gate[expert], preferred_element_type=jnp.float32)
        up_val = jnp.dot(expert_rows, w_up[expert], preferred_element_type=jnp.float32)
        hidden = (jax.nn.silu(gate_val) * up_val).astype(jnp.bfloat16)
        summed = jnp.zeros((max_rows, D), jnp.float32)
        for shard_index in range(N_TP):
            block_out = jnp.dot(hidden[:, shard_index * ff_shard:(shard_index + 1) * ff_shard], w_down[expert, shard_index * ff_shard:(shard_index + 1) * ff_shard], preferred_element_type=jnp.float32).astype(jnp.bfloat16)
            summed = summed + lax.optimization_barrier(block_out).astype(jnp.float32)
        expert_out = lax.optimization_barrier(summed.astype(jnp.bfloat16)).astype(jnp.float32)
        weight = flat_weight[picked] * is_valid
        layer_sum = layer_sum.at[token_index].add(weight[:, None] * expert_out)
        return (layer_sum, None)
    expert_total, unused = lax.scan(one_expert, jnp.zeros((TOKENS, D), jnp.float32), jnp.arange(EXPERTS).astype(jnp.int32))
    return (after_f32 + expert_total).astype(jnp.bfloat16)
```

```python
import functools

import jax
import jax.numpy as jnp
from jax import lax
from jax.experimental import pallas as pl
from jax.experimental.pallas import tpu as pltpu
from jax.sharding import PartitionSpec as P

NORM_EPS = 1e-06


MESH = pl.DeviceIdType.MESH
COL_TILE = 256
LANES = 2
CHUNKS = 8
SPREAD_AHEAD = 3
PASS_AHEAD = 1
SIDE_LAG = 2


def as_rows(block):
    width = block.shape[-1]
    if block.shape[-2] % 16:
        return block.astype(jnp.float32).reshape(-1, width).astype(block.dtype)
    return block.reshape(-1, width)


def flip(code, sp_count):
    return jnp.where(code == 0, 0, sp_count - code)


def turned(me, code, sp_count):
    if sp_count != 4 * LANES:
        return code
    inside = ((me // LANES == 1) | (me // LANES == 2)) & (code >= sp_count // 2)
    return jnp.where(inside, code ^ LANES, code)


def step_of(peer, me, sp_count):
    return flip(turned(me, peer ^ me, sp_count), sp_count)


def peer_of(step, me, sp_count):
    return turned(me, flip(step, sp_count), sp_count) ^ me


def as_column(row):
    size = row.shape[1]
    rows = lax.broadcasted_iota(jnp.int32, (size, size), 0)
    columns = lax.broadcasted_iota(jnp.int32, (size, size), 1)
    return jnp.sum(jnp.where(rows == columns, row, 0.0), axis=1, keepdims=True)


def as_row(column):
    size = column.shape[0]
    rows = lax.broadcasted_iota(jnp.int32, (size, size), 0)
    columns = lax.broadcasted_iota(jnp.int32, (size, size), 1)
    return jnp.sum(jnp.where(rows == columns, column, 0.0), axis=0, keepdims=True)


def chunk_count(sp_count):
    return CHUNKS if sp_count % CHUNKS == 0 else sp_count


def col_tile(width):
    return COL_TILE if width % COL_TILE == 0 else width


def expert_kernel(
    sp_count,
    tp_count,
    cap,
    stream_ref,
    mix_ref,
    pool_ref,
    scale_ref,
    gain_ref,
    routes_ref,
    weight_ref,
    gate_hbm,
    up_hbm,
    down_hbm,
    out_ref,
    squares,
    squares2,
    routes_all,
    tail,
    halo,
    mixed,
    tokens,
    picked_at,
    send_ref,
    gate,
    up,
    down,
    arrived,
    hidden,
    partial,
    pair_in,
    pair_sum,
    side_in,
    served,
    returned,
    round_sem,
    square_sem,
    square2_sem,
    route_sem,
    halo_sem,
    token_sem,
    local_sem,
    first_send,
    first_recv,
    side_send,
    side_recv,
    pair_send,
    pair_recv,
    back_pair,
    back_side,
    back_send,
    back_recv,
):
    me = lax.axis_index("sp")
    tp_me = lax.axis_index("tp")
    high, low = tp_me // LANES, lax.rem(tp_me, LANES)
    highs = tp_count // LANES
    other_low = 1 - low
    pair_id = {"sp": me, "tp": high * LANES + other_low}
    pairs_count = sp_count // LANES
    chunks = chunk_count(sp_count)
    group = sp_count // chunks
    ff_width = gate.shape[1]
    tok_rows, group_width = stream_ref.shape
    width = group_width * tp_count
    halo_rows = halo.shape[0]
    tok_count = tokens.shape[1]
    top_count = routes_ref.shape[0]
    slot_count = sp_count * cap
    chunk_rows = hidden.shape[0]

    def side_high(distance):
        return lax.rem(high + distance, highs)

    def side_id(distance):
        return {"sp": me, "tp": side_high(distance) * LANES + low}

    def from_high(distance):
        return lax.rem(high - distance + highs, highs)

    def tp_id(distance):
        return {"sp": me, "tp": lax.rem(tp_me + distance, tp_count)}

    def sp_id(peer):
        return {"sp": peer, "tp": tp_me}

    def columns_of(piece):
        return pl.ds(pl.multiple_of(piece * group_width, group_width), group_width)

    weight_copies = [
        pltpu.make_async_copy(source.at[0], target, local_sem.at[index])
        for index, (source, target) in enumerate(((gate_hbm, gate), (up_hbm, up), (down_hbm, down)))
    ]
    for copy in weight_copies:
        copy.start()

    barrier = pltpu.get_barrier_semaphore()
    beside = me ^ 1
    across = jnp.where(lax.rem(me, LANES) == 1, me + 1, me - 1)
    has_across = (across >= 0) & (across < sp_count)
    has_up = me + LANES < sp_count
    has_down = me - LANES >= 0
    near_count = 1 + has_up.astype(jnp.int32) + has_down.astype(jnp.int32)

    def tell_near(sem):
        pl.semaphore_signal(sem, inc=1, device_id=sp_id(beside), device_id_type=MESH)

        @pl.when(has_up)
        def _():
            pl.semaphore_signal(sem, inc=1, device_id=sp_id(me + LANES), device_id_type=MESH)

        @pl.when(has_down)
        def _():
            pl.semaphore_signal(sem, inc=1, device_id=sp_id(me - LANES), device_id_type=MESH)

    for distance in range(1, tp_count):
        pl.semaphore_signal(barrier, inc=1, device_id=tp_id(distance), device_id_type=MESH)

    @pl.when(has_across)
    def _():
        pl.semaphore_signal(barrier, inc=1, device_id=sp_id(across), device_id_type=MESH)

    tell_near(barrier)

    def square_copy(distance):
        return pltpu.make_async_remote_copy(
            src_ref=squares.at[0],
            dst_ref=squares.at[distance],
            send_sem=square_sem.at[0, distance - 1],
            recv_sem=square_sem.at[1, distance - 1],
            device_id=tp_id(distance),
            device_id_type=MESH,
        )

    def square2_copy(distance):
        return pltpu.make_async_remote_copy(
            src_ref=squares2.at[0],
            dst_ref=squares2.at[distance],
            send_sem=square2_sem.at[0, distance - 1],
            recv_sem=square2_sem.at[1, distance - 1],
            device_id=tp_id(distance),
            device_id_type=MESH,
        )

    def route_copy(distance):
        return pltpu.make_async_remote_copy(
            src_ref=routes_ref,
            dst_ref=routes_all.at[tp_me],
            send_sem=route_sem.at[0, distance - 1],
            recv_sem=route_sem.at[1, distance - 1],
            device_id=tp_id(distance),
            device_id_type=MESH,
        )

    halo_copy = pltpu.make_async_remote_copy(
        src_ref=tail,
        dst_ref=halo,
        send_sem=halo_sem.at[0],
        recv_sem=halo_sem.at[1],
        device_id=sp_id(me + 1),
        device_id_type=MESH,
    )

    def token_copy(distance):
        return pltpu.make_async_remote_copy(
            src_ref=mixed.at[lax.rem(tp_me + distance, tp_count)],
            dst_ref=tokens.at[tp_me],
            send_sem=token_sem.at[0, distance - 1],
            recv_sem=token_sem.at[1, distance - 1],
            device_id=tp_id(distance),
            device_id_type=MESH,
        )

    stream_f32 = stream_ref[...].astype(jnp.float32)
    own_square = as_row(jnp.sum(stream_f32 * stream_f32, axis=1, keepdims=True))
    squares[0] = jnp.broadcast_to(own_square, squares.shape[1:])
    pl.semaphore_wait(barrier, tp_count - 1 + near_count + has_across.astype(jnp.int32))
    for distance in range(1, tp_count):
        square_copy(distance).start()
    for distance in range(1, tp_count):
        route_copy(distance).start()
    if pairs_count > 1:
        tell_near(round_sem.at[0])
    routes_all[tp_me] = routes_ref[...]

    window_len = jnp.left_shift(jnp.int32(2), tp_me)
    first_row = me * tok_rows
    row_at = lax.broadcasted_iota(jnp.int32, (tok_rows, tok_rows), 0)
    source_at = lax.broadcasted_iota(jnp.int32, (tok_rows, tok_rows), 1)
    lag = row_at - source_at
    band = jnp.where((lag >= 0) & (lag < window_len), 1.0, 0.0).astype(jnp.bfloat16)
    row_at = lax.broadcasted_iota(jnp.int32, (halo_rows, halo_rows), 0)
    source_at = lax.broadcasted_iota(jnp.int32, (halo_rows, halo_rows), 1) - halo_rows
    reach = (row_at - source_at < window_len) & (first_row + source_at >= 0)
    halo_band = jnp.where(reach, 1.0, 0.0).astype(jnp.bfloat16)
    position = first_row + lax.broadcasted_iota(jnp.int32, (tok_rows, 1), 0)
    window_count = jnp.minimum(position + 1, window_len).astype(jnp.float32)
    pool_scale = scale_ref[...].astype(jnp.float32)[None, :]

    for distance in range(1, tp_count):
        square_copy(distance).wait_recv()
    square = squares[0, 0:1, :]
    for distance in range(1, tp_count):
        square = square + squares[distance, 0:1, :]
    row_scale = lax.rsqrt(as_column(square) / width + NORM_EPS)
    normed = stream_f32 * row_scale * mix_ref[...].astype(jnp.float32)[None, :]
    normed = normed.astype(jnp.bfloat16)
    tail[...] = normed[tok_rows - halo_rows :]

    @pl.when(me + 1 < sp_count)
    def _():
        halo_copy.start()

    def mix(sums, counts, own, rows):
        pooled = (sums / counts - own.astype(jnp.float32)).astype(jnp.bfloat16)
        mixer_out = jnp.dot(pooled, pool_ref[0], preferred_element_type=jnp.float32)
        return (rows + mixer_out * pool_scale).astype(jnp.bfloat16)

    window_sum = jnp.dot(band, normed, preferred_element_type=jnp.float32)
    after_mix = mix(window_sum, window_count, normed, stream_f32)
    for piece in range(tp_count):
        mixed[piece] = after_mix[piece * tok_count : (piece + 1) * tok_count]

    def next_round(index):
        pl.semaphore_wait(round_sem.at[index], near_count)
        if index + 2 < pairs_count:
            tell_near(round_sem.at[index + 1])

    if pairs_count > 1:
        next_round(0)

    @pl.when(me > 0)
    def _():
        halo_copy.wait_recv()

    @pl.when(me == 0)
    def _():
        halo[...] = jnp.zeros_like(halo)

    first_sum = window_sum[:halo_rows]
    first_sum = first_sum + jnp.dot(halo_band, halo[...], preferred_element_type=jnp.float32)
    first_mix = mix(
        first_sum, window_count[:halo_rows], normed[:halo_rows], stream_f32[:halo_rows]
    )
    mixed[0, 0:halo_rows, :] = first_mix
    after_f32 = mixed[...].reshape(tok_rows, group_width).astype(jnp.float32)
    own_square = as_row(jnp.sum(after_f32 * after_f32, axis=1, keepdims=True))
    squares2[0] = jnp.broadcast_to(own_square, squares2.shape[1:])
    for distance in range(1, tp_count):
        square2_copy(distance).start()
    for distance in range(1, tp_count):
        token_copy(distance).start()
    tokens[tp_me] = mixed[tp_me]

    if pairs_count > 2:
        next_round(1)

    experts = lax.broadcasted_iota(jnp.int32, (128, tok_count), 0)
    earlier = lax.broadcasted_iota(jnp.int32, (tok_count, tok_count), 0)
    later = lax.broadcasted_iota(jnp.int32, (tok_count, tok_count), 1)
    before = jnp.where(earlier < later, 1.0, 0.0).astype(jnp.bfloat16)
    slots = lax.broadcasted_iota(jnp.int32, (slot_count, tok_count), 0).astype(jnp.float32)
    for distance in range(1, tp_count):
        route_copy(distance).wait_recv()
    for piece in range(tp_count):
        routes = routes_all[piece]
        named = [experts == routes[pick : pick + 1, :] for pick in range(top_count)]
        hits = named[0].astype(jnp.float32)
        for pick in range(1, top_count):
            hits = hits + named[pick].astype(jnp.float32)
        rank = jnp.dot(hits.astype(jnp.bfloat16), before, preferred_element_type=jnp.float32)
        for pick in range(top_count):
            start = step_of(routes[pick : pick + 1, :], me, sp_count) * cap
            spot = jnp.sum(jnp.where(named[pick], rank, 0.0), axis=0, keepdims=True)
            spot = spot + start.astype(jnp.float32)
            picked_at[piece, pick] = jnp.where(slots == spot, 1.0, 0.0).astype(jnp.bfloat16)
    gain = gain_ref[0:group_width]
    for piece in range(1, tp_count):
        columns = slice(piece * group_width, (piece + 1) * group_width)
        gain = jnp.where(tp_me == piece, gain_ref[columns], gain)
    gain = gain.astype(jnp.float32)[None, :]

    for distance in range(1, tp_count):
        square2_copy(distance).wait_recv()
    square = squares2[0, 0:1, :]
    for distance in range(1, tp_count):
        square = square + squares2[distance, 0:1, :]
    ffn_scale = lax.rsqrt(as_column(square) / width + NORM_EPS)
    normed2 = (after_f32 * ffn_scale * gain).astype(jnp.bfloat16)
    for index in range(2, pairs_count - 1):
        next_round(index)
    for piece in range(tp_count):
        dispatch = picked_at[piece, 0]
        for pick in range(1, top_count):
            dispatch = dispatch + picked_at[piece, pick]
        rows = jnp.dot(
            dispatch,
            normed2[piece * tok_count : (piece + 1) * tok_count],
            preferred_element_type=jnp.float32,
        )
        rows = rows.reshape(sp_count, cap, group_width).astype(jnp.bfloat16)
        send_ref[:, piece % LANES, piece // LANES] = rows

    def first_copy(step):
        peer = peer_of(step, me, sp_count)
        return pltpu.make_async_remote_copy(
            src_ref=send_ref.at[step],
            dst_ref=arrived.at[step_of(me, peer, sp_count), :, :, :, columns_of(tp_me)],
            send_sem=first_send.at[step],
            recv_sem=first_recv.at[step_of(me, peer, sp_count)],
            device_id=sp_id(peer),
            device_id_type=MESH,
        )

    def first_arrival(step):
        return pltpu.make_async_remote_copy(
            src_ref=send_ref.at[step],
            dst_ref=arrived.at[step, :, :, :, columns_of(tp_me)],
            send_sem=first_send.at[step],
            recv_sem=first_recv.at[step],
            device_id=sp_id(peer_of(step, me, sp_count)),
            device_id_type=MESH,
        )

    def side_copy(step, distance):
        block = arrived.at[step, :, :, :, columns_of(tp_me)]
        return pltpu.make_async_remote_copy(
            src_ref=block,
            dst_ref=block,
            send_sem=side_send.at[step, distance - 1],
            recv_sem=side_recv.at[step, distance - 1],
            device_id=side_id(distance),
            device_id_type=MESH,
        )

    def pair_copy(step, distance):
        piece = from_high(distance) * LANES + low
        block = arrived.at[step, :, :, :, columns_of(piece)]
        return pltpu.make_async_remote_copy(
            src_ref=block,
            dst_ref=block,
            send_sem=pair_send.at[step, distance],
            recv_sem=pair_recv.at[step, distance],
            device_id=pair_id,
            device_id_type=MESH,
        )

    def steps_of(chunk):
        return [chunk * group + index for index in range(group)]

    def share(step):
        for distance in range(1, highs):
            side_copy(step, distance).start()
        pair_copy(step, 0).start()

    def spread(chunk):
        for step in steps_of(chunk):
            if not (isinstance(step, int) and step == 0):
                first_arrival(step).wait_recv()
            share(step)

    def pass_on(chunk):
        for step in steps_of(chunk):
            for distance in range(1, highs):
                side_copy(step, distance).wait_recv()
                pair_copy(step, distance).start()

    def settle(chunk):
        for step in steps_of(chunk):
            for distance in range(highs):
                pair_copy(step, distance).wait_recv()

    def span(chunk):
        return pl.ds(chunk * group, group)

    tile = col_tile(ff_width)
    tiles = ff_width // tile
    out_tile = col_tile(width)

    def gate_up(chunk, first, last):
        rows = as_rows(arrived[span(chunk)])
        for index in range(first, last):
            columns = slice(index * tile, (index + 1) * tile)
            gate_val = jnp.dot(rows, gate[:, columns], preferred_element_type=jnp.float32)
            up_val = jnp.dot(rows, up[:, columns], preferred_element_type=jnp.float32)
            hidden[:, columns] = (jax.nn.silu(gate_val) * up_val).astype(jnp.bfloat16)

    def project(chunk):
        for index in range(width // out_tile):
            columns = slice(index * out_tile, (index + 1) * out_tile)
            block = jnp.dot(hidden[...], down[:, columns], preferred_element_type=jnp.float32)
            block = block.reshape(group, LANES, highs, cap, out_tile).astype(jnp.bfloat16)
            partial[span(chunk), :, :, :, columns] = block

    def back_pair_copy(chunk):
        return pltpu.make_async_remote_copy(
            src_ref=partial.at[span(chunk), other_low],
            dst_ref=pair_in.at[span(chunk)],
            send_sem=back_pair.at[0, chunk],
            recv_sem=back_pair.at[1, chunk],
            device_id=pair_id,
            device_id_type=MESH,
        )

    def back_side_copy(chunk, distance):
        return pltpu.make_async_remote_copy(
            src_ref=pair_sum.at[distance - 1, span(chunk)],
            dst_ref=side_in.at[distance - 1, span(chunk)],
            send_sem=back_side.at[0, chunk, distance - 1],
            recv_sem=back_side.at[1, chunk, distance - 1],
            device_id=side_id(distance),
            device_id_type=MESH,
        )

    def back_copy(step):
        peer = peer_of(step, me, sp_count)
        return pltpu.make_async_remote_copy(
            src_ref=served.at[step],
            dst_ref=returned.at[step_of(me, peer, sp_count)],
            send_sem=back_send.at[step],
            recv_sem=back_recv.at[step_of(me, peer, sp_count)],
            device_id=sp_id(peer),
            device_id_type=MESH,
        )

    def back_arrival(step):
        return pltpu.make_async_remote_copy(
            src_ref=served.at[step],
            dst_ref=returned.at[step],
            send_sem=back_send.at[step],
            recv_sem=back_recv.at[step],
            device_id=sp_id(peer_of(step, me, sp_count)),
            device_id_type=MESH,
        )

    def pair_add(chunk):
        back_pair_copy(chunk).wait_recv()
        for distance in range(1, highs):
            target = side_high(distance)
            for step in steps_of(chunk):
                total = partial[step, low, target].astype(jnp.float32)
                total = total + pair_in[step, target].astype(jnp.float32)
                pair_sum[distance - 1, step] = total.astype(jnp.bfloat16)
            back_side_copy(chunk, distance).start()

    def side_add(chunk):
        for distance in range(1, highs):
            back_side_copy(chunk, distance).wait_recv()
        for step in steps_of(chunk):
            total = partial[step, low, high].astype(jnp.float32)
            total = total + pair_in[step, high].astype(jnp.float32)
            for distance in range(1, highs):
                total = total + side_in[distance - 1, step].astype(jnp.float32)
            total = total.astype(jnp.bfloat16)

            def keep(step=step, total=total):
                returned[step] = total

            def give(step=step, total=total):
                served[step] = total
                back_copy(step).start()

            if isinstance(step, int):
                (keep if step == 0 else give)()
            else:
                pl.when(step == 0)(keep)
                pl.when(step > 0)(give)

    for step in range(1, sp_count):
        first_copy(step).start()
    arrived[0, :, :, :, columns_of(tp_me)] = send_ref[0]

    for chunk in range(min(SPREAD_AHEAD, chunks)):
        spread(chunk)
    for chunk in range(min(PASS_AHEAD, chunks)):
        pass_on(chunk)
    for copy in weight_copies:
        copy.wait()
    early = (tiles + 1) // 2

    def turn(chunk, carry):
        settle(chunk)
        gate_up(chunk, 0, early)

        @pl.when(chunk >= 1)
        def _():
            pair_add(chunk - 1)

        @pl.when(chunk + SPREAD_AHEAD < chunks)
        def _():
            spread(chunk + SPREAD_AHEAD)

        gate_up(chunk, early, tiles)

        @pl.when(chunk + PASS_AHEAD < chunks)
        def _():
            pass_on(chunk + PASS_AHEAD)

        @pl.when(chunk >= SIDE_LAG)
        def _():
            side_add(chunk - SIDE_LAG)

        project(chunk)
        back_pair_copy(chunk).start()
        return carry

    lax.fori_loop(0, chunks, turn, 0)
    pair_add(chunks - 1)
    for chunk in range(max(0, chunks - SIDE_LAG), chunks):
        side_add(chunk)

    for distance in range(1, tp_count):
        token_copy(distance).wait_recv()
    for step in range(1, sp_count):
        back_arrival(step).wait_recv()
    rows = as_rows(returned[...])
    route_weights = [as_column(weight_ref[pick : pick + 1, :]) for pick in range(top_count)]
    for piece in range(tp_count):
        columns = slice(piece * group_width, (piece + 1) * group_width)
        total = tokens[piece].astype(jnp.float32)
        for pick in range(top_count):
            picked = lax.dot_general(
                picked_at[tp_me, pick],
                rows[:, columns],
                (((0,), (0,)), ((), ())),
                preferred_element_type=jnp.float32,
            )
            total = total + route_weights[pick] * picked
        out_ref[:, columns] = total.astype(jnp.bfloat16)

    @pl.when(me + 1 < sp_count)
    def _():
        halo_copy.wait_send()

    for distance in range(1, tp_count):
        square_copy(distance).wait_send()
        square2_copy(distance).wait_send()
        route_copy(distance).wait_send()
        token_copy(distance).wait_send()

    def finish(step, carry):
        for distance in range(1, highs):
            side_copy(step, distance).wait_send()
        for distance in range(highs):
            pair_copy(step, distance).wait_send()
        return carry

    def finish_far(step, carry):
        first_copy(step).wait_send()
        back_copy(step).wait_send()
        return carry

    def finish_back(chunk, carry):
        back_pair_copy(chunk).wait_send()
        for distance in range(1, highs):
            back_side_copy(chunk, distance).wait_send()
        return carry

    lax.fori_loop(0, sp_count, finish, 0)
    lax.fori_loop(1, sp_count, finish_far, 0)
    lax.fori_loop(0, chunks, finish_back, 0)


def per_device(
    stream, mix_gain, pool_weight, pool_scale, ffn_gain, routes, route_weight, w_gate, w_up, w_down
):
    tok_rows, group_width = stream.shape
    tp_count = lax.axis_size("tp")
    sp_count = lax.axis_size("sp")
    width = group_width * tp_count
    tok_count, top_count = routes.shape
    cap = 2 * tok_count * top_count // sp_count
    halo_rows = 2 ** (pool_weight.shape[0] * tp_count)
    highs = tp_count // LANES
    chunks = chunk_count(sp_count)
    chunk_rows = sp_count // chunks * tp_count * cap
    ff_width = w_gate.shape[2]
    half = jnp.bfloat16
    vmem = pl.BlockSpec(memory_space=pltpu.VMEM)
    hbm = pl.BlockSpec(memory_space=pl.ANY)
    dma = pltpu.SemaphoreType.DMA
    rounds = max(1, sp_count // LANES - 1)
    return pl.pallas_call(
        functools.partial(expert_kernel, sp_count, tp_count, cap),
        out_shape=jax.ShapeDtypeStruct((tok_count, width), half),
        in_specs=[vmem] * 7 + [hbm] * 3,
        out_specs=vmem,
        scratch_shapes=[
            pltpu.VMEM((tp_count, 8, tok_rows), jnp.float32),
            pltpu.VMEM((tp_count, 8, tok_rows), jnp.float32),
            pltpu.VMEM((tp_count, top_count, tok_count), jnp.int32),
            pltpu.VMEM((halo_rows, group_width), half),
            pltpu.VMEM((halo_rows, group_width), half),
            pltpu.VMEM((tp_count, tok_count, group_width), half),
            pltpu.VMEM((tp_count, tok_count, group_width), half),
            pltpu.VMEM((tp_count, top_count, sp_count * cap, tok_count), half),
            pltpu.VMEM((sp_count, LANES, highs, cap, group_width), half),
            pltpu.VMEM(w_gate.shape[1:], half),
            pltpu.VMEM(w_up.shape[1:], half),
            pltpu.VMEM(w_down.shape[1:], half),
            pltpu.VMEM((sp_count, LANES, highs, cap, width), half),
            pltpu.VMEM((chunk_rows, ff_width), half),
            pltpu.VMEM((sp_count, LANES, highs, cap, width), half),
            pltpu.VMEM((sp_count, highs, cap, width), half),
            pltpu.VMEM((highs - 1, sp_count, cap, width), half),
            pltpu.VMEM((highs - 1, sp_count, cap, width), half),
            pltpu.VMEM((sp_count, cap, width), half),
            pltpu.VMEM((sp_count, cap, width), half),
            pltpu.SemaphoreType.REGULAR((rounds,)),
            dma((2, tp_count - 1)),
            dma((2, tp_count - 1)),
            dma((2, tp_count - 1)),
            dma((2,)),
            dma((2, tp_count - 1)),
            dma((3,)),
            dma((sp_count,)),
            dma((sp_count,)),
            dma((sp_count, highs - 1)),
            dma((sp_count, highs - 1)),
            dma((sp_count, highs)),
            dma((sp_count, highs)),
            dma((2, chunks)),
            dma((2, chunks, highs - 1)),
            dma((sp_count,)),
            dma((sp_count,)),
        ],
        compiler_params=pltpu.CompilerParams(
            collective_id=1, has_side_effects=True, vmem_limit_bytes=60 * 1024 * 1024
        ),
    )(
        stream,
        mix_gain,
        pool_weight,
        pool_scale,
        ffn_gain,
        routes.T,
        route_weight.T,
        w_gate,
        w_up,
        w_down,
    )


def solution(mesh):
    in_specs = (
        P("sp", "tp"),
        P("tp"),
        P("tp", None, None),
        P("tp"),
        P(),
        P(("sp", "tp"), None),
        P(("sp", "tp"), None),
        P("sp", None, "tp"),
        P("sp", None, "tp"),
        P("sp", "tp", None),
    )
    out_specs = P(("sp", "tp"), None)
    return jax.shard_map(
        per_device, mesh=mesh, in_specs=in_specs, out_specs=out_specs, check_vma=False
    )
```

```python
import functools

import jax
import jax.numpy as jnp
from jax import lax
from jax.experimental import pallas as pl
from jax.experimental.pallas import tpu as pltpu
from jax.sharding import PartitionSpec as P

NORM_EPS = 1e-06


MESH = pl.DeviceIdType.MESH
COL_TILE = 256
LANES = 2
CHUNKS = 8
SPREAD_AHEAD = 3
PASS_AHEAD = 1
SIDE_LAG = 3
NEAR = 4
ORDER = (0, 7, 6, 3, 5, 2, 4, 1)
ISSUE = (1, 2, 4, 6, 3, 5, 7)


def as_rows(block):
    width = block.shape[-1]
    if block.shape[-2] % 16:
        return block.astype(jnp.float32).reshape(-1, width).astype(block.dtype)
    return block.reshape(-1, width)


def ranked(sp_count):
    if sp_count == len(ORDER):
        return ORDER
    return tuple(range(sp_count))


def looked_up(table, index):
    found = jnp.zeros_like(index)
    for key, value in enumerate(table):
        found = jnp.where(index == key, value, found)
    return found


def code_of(step, sp_count):
    table = ranked(sp_count)
    if isinstance(step, int):
        return jnp.int32(table[step])
    return looked_up(table, step)


def turned(me, code, sp_count):
    if sp_count != 4 * LANES:
        return code
    inside = ((me // LANES == 1) | (me // LANES == 2)) & (code >= sp_count // 2)
    return jnp.where(inside, code ^ LANES, code)


def step_of(peer, me, sp_count):
    table = ranked(sp_count)
    places = [table.index(code) for code in range(sp_count)]
    return looked_up(places, turned(me, peer ^ me, sp_count))


def peer_of(step, me, sp_count):
    return turned(me, code_of(step, sp_count), sp_count) ^ me


def as_column(row):
    size = row.shape[1]
    rows = lax.broadcasted_iota(jnp.int32, (size, size), 0)
    columns = lax.broadcasted_iota(jnp.int32, (size, size), 1)
    return jnp.sum(jnp.where(rows == columns, row, 0.0), axis=1, keepdims=True)


def as_row(column):
    size = column.shape[0]
    rows = lax.broadcasted_iota(jnp.int32, (size, size), 0)
    columns = lax.broadcasted_iota(jnp.int32, (size, size), 1)
    return jnp.sum(jnp.where(rows == columns, column, 0.0), axis=0, keepdims=True)


def chunk_count(sp_count):
    return CHUNKS if sp_count % CHUNKS == 0 else sp_count


def col_tile(width):
    return COL_TILE if width % COL_TILE == 0 else width


def expert_kernel(
    sp_count,
    tp_count,
    cap,
    stream_ref,
    mix_ref,
    pool_ref,
    scale_ref,
    gain_ref,
    routes_ref,
    weight_ref,
    gate_hbm,
    up_hbm,
    down_hbm,
    out_ref,
    squares,
    squares2,
    routes_all,
    tail,
    halo,
    mixed,
    mixed_far,
    tokens,
    picked_at,
    send_ref,
    send_near,
    gate,
    up,
    down,
    arrived,
    hidden,
    partial,
    pair_in,
    pair_sum,
    side_in,
    served,
    returned,
    round_sem,
    square_sem,
    square2_sem,
    route_sem,
    halo_sem,
    raw_sem,
    token_sem,
    local_sem,
    first_send,
    first_recv,
    near_send,
    side_send,
    side_recv,
    pair_send,
    pair_recv,
    back_pair,
    back_side,
    back_send,
    back_recv,
):
    me = lax.axis_index("sp")
    tp_me = lax.axis_index("tp")
    high, low = tp_me // LANES, lax.rem(tp_me, LANES)
    highs = tp_count // LANES
    other_low = 1 - low
    pair_id = {"sp": me, "tp": high * LANES + other_low}
    pairs_count = sp_count // LANES
    chunks = chunk_count(sp_count)
    group = sp_count // chunks
    ff_width = gate.shape[1]
    tok_rows, group_width = stream_ref.shape
    width = group_width * tp_count
    halo_rows = halo.shape[0]
    tok_count = tokens.shape[1]
    top_count = routes_ref.shape[0]
    slot_count = sp_count * cap
    chunk_rows = hidden.shape[0]

    def side_high(distance):
        return lax.rem(high + distance, highs)

    def side_id(distance):
        return {"sp": me, "tp": side_high(distance) * LANES + low}

    def from_high(distance):
        return lax.rem(high - distance + highs, highs)

    def tp_id(distance):
        return {"sp": me, "tp": lax.rem(tp_me + distance, tp_count)}

    def sp_id(peer):
        return {"sp": peer, "tp": tp_me}

    def columns_of(piece):
        return pl.ds(pl.multiple_of(piece * group_width, group_width), group_width)

    weight_copies = [
        pltpu.make_async_copy(source.at[0], target, local_sem.at[index])
        for index, (source, target) in enumerate(((gate_hbm, gate), (up_hbm, up), (down_hbm, down)))
    ]
    for copy in weight_copies:
        copy.start()

    barrier = pltpu.get_barrier_semaphore()
    beside = me ^ 1
    across = jnp.where(lax.rem(me, LANES) == 1, me + 1, me - 1)
    has_across = (across >= 0) & (across < sp_count)
    has_up = me + LANES < sp_count
    has_down = me - LANES >= 0
    near_count = 1 + has_up.astype(jnp.int32) + has_down.astype(jnp.int32)

    def tell_near(sem):
        pl.semaphore_signal(sem, inc=1, device_id=sp_id(beside), device_id_type=MESH)

        @pl.when(has_up)
        def _():
            pl.semaphore_signal(sem, inc=1, device_id=sp_id(me + LANES), device_id_type=MESH)

        @pl.when(has_down)
        def _():
            pl.semaphore_signal(sem, inc=1, device_id=sp_id(me - LANES), device_id_type=MESH)

    for distance in range(1, tp_count):
        pl.semaphore_signal(barrier, inc=1, device_id=tp_id(distance), device_id_type=MESH)

    @pl.when(has_across)
    def _():
        pl.semaphore_signal(barrier, inc=1, device_id=sp_id(across), device_id_type=MESH)

    tell_near(barrier)

    def square_copy(distance):
        return pltpu.make_async_remote_copy(
            src_ref=squares.at[0],
            dst_ref=squares.at[distance],
            send_sem=square_sem.at[0, distance - 1],
            recv_sem=square_sem.at[1, distance - 1],
            device_id=tp_id(distance),
            device_id_type=MESH,
        )

    def square2_copy(distance):
        return pltpu.make_async_remote_copy(
            src_ref=squares2.at[0],
            dst_ref=squares2.at[distance],
            send_sem=square2_sem.at[0, distance - 1],
            recv_sem=square2_sem.at[1, distance - 1],
            device_id=tp_id(distance),
            device_id_type=MESH,
        )

    def route_copy(distance):
        return pltpu.make_async_remote_copy(
            src_ref=routes_ref,
            dst_ref=routes_all.at[tp_me],
            send_sem=route_sem.at[0, distance - 1],
            recv_sem=route_sem.at[1, distance - 1],
            device_id=tp_id(distance),
            device_id_type=MESH,
        )

    halo_copy = pltpu.make_async_remote_copy(
        src_ref=tail,
        dst_ref=halo,
        send_sem=halo_sem.at[0],
        recv_sem=halo_sem.at[1],
        device_id=sp_id(me + 1),
        device_id_type=MESH,
    )

    def far_piece(distance):
        return from_high(distance) * LANES + low

    def raw_copy(distance):
        return pltpu.make_async_remote_copy(
            src_ref=mixed,
            dst_ref=mixed_far.at[distance - 1],
            send_sem=raw_sem.at[0, distance - 1],
            recv_sem=raw_sem.at[1, distance - 1],
            device_id=side_id(distance),
            device_id_type=MESH,
        )

    def token_copy(distance):
        block = high * LANES + other_low
        source = mixed.at[block] if distance == 0 else mixed_far.at[distance - 1, block]
        return pltpu.make_async_remote_copy(
            src_ref=source,
            dst_ref=tokens.at[far_piece(distance)],
            send_sem=token_sem.at[0, distance],
            recv_sem=token_sem.at[1, distance],
            device_id=pair_id,
            device_id_type=MESH,
        )

    stream_f32 = stream_ref[...].astype(jnp.float32)
    own_square = as_row(jnp.sum(stream_f32 * stream_f32, axis=1, keepdims=True))
    squares[0] = jnp.broadcast_to(own_square, squares.shape[1:])
    pl.semaphore_wait(barrier, tp_count - 1 + near_count + has_across.astype(jnp.int32))
    for distance in range(1, tp_count):
        square_copy(distance).start()
    for distance in range(1, tp_count):
        route_copy(distance).start()
    if pairs_count > 1:
        tell_near(round_sem.at[0])
    routes_all[tp_me] = routes_ref[...]

    window_len = jnp.left_shift(jnp.int32(2), tp_me)
    first_row = me * tok_rows
    row_at = lax.broadcasted_iota(jnp.int32, (tok_rows, tok_rows), 0)
    source_at = lax.broadcasted_iota(jnp.int32, (tok_rows, tok_rows), 1)
    lag = row_at - source_at
    band = jnp.where((lag >= 0) & (lag < window_len), 1.0, 0.0).astype(jnp.bfloat16)
    row_at = lax.broadcasted_iota(jnp.int32, (halo_rows, halo_rows), 0)
    source_at = lax.broadcasted_iota(jnp.int32, (halo_rows, halo_rows), 1) - halo_rows
    reach = (row_at - source_at < window_len) & (first_row + source_at >= 0)
    halo_band = jnp.where(reach, 1.0, 0.0).astype(jnp.bfloat16)
    position = first_row + lax.broadcasted_iota(jnp.int32, (tok_rows, 1), 0)
    window_count = jnp.minimum(position + 1, window_len).astype(jnp.float32)
    pool_scale = scale_ref[...].astype(jnp.float32)[None, :]

    for distance in range(1, tp_count):
        square_copy(distance).wait_recv()
    square = squares[0, 0:1, :]
    for distance in range(1, tp_count):
        square = square + squares[distance, 0:1, :]
    row_scale = lax.rsqrt(as_column(square) / width + NORM_EPS)
    normed = stream_f32 * row_scale * mix_ref[...].astype(jnp.float32)[None, :]
    normed = normed.astype(jnp.bfloat16)
    tail[...] = normed[tok_rows - halo_rows :]

    @pl.when(me + 1 < sp_count)
    def _():
        halo_copy.start()

    def mix(sums, counts, own, rows):
        pooled = (sums / counts - own.astype(jnp.float32)).astype(jnp.bfloat16)
        mixer_out = jnp.dot(pooled, pool_ref[0], preferred_element_type=jnp.float32)
        return (rows + mixer_out * pool_scale).astype(jnp.bfloat16)

    window_sum = jnp.dot(band, normed, preferred_element_type=jnp.float32)
    after_mix = mix(window_sum, window_count, normed, stream_f32)
    for piece in range(tp_count):
        mixed[piece] = after_mix[piece * tok_count : (piece + 1) * tok_count]

    def next_round(index):
        pl.semaphore_wait(round_sem.at[index], near_count)
        if index + 2 < pairs_count:
            tell_near(round_sem.at[index + 1])

    if pairs_count > 1:
        next_round(0)

    @pl.when(me > 0)
    def _():
        halo_copy.wait_recv()

    @pl.when(me == 0)
    def _():
        halo[...] = jnp.zeros_like(halo)

    first_sum = window_sum[:halo_rows]
    first_sum = first_sum + jnp.dot(halo_band, halo[...], preferred_element_type=jnp.float32)
    first_mix = mix(
        first_sum, window_count[:halo_rows], normed[:halo_rows], stream_f32[:halo_rows]
    )
    mixed[0, 0:halo_rows, :] = first_mix
    after_f32 = mixed[...].reshape(tok_rows, group_width).astype(jnp.float32)
    own_square = as_row(jnp.sum(after_f32 * after_f32, axis=1, keepdims=True))
    squares2[0] = jnp.broadcast_to(own_square, squares2.shape[1:])
    for distance in range(1, tp_count):
        square2_copy(distance).start()
    for distance in range(1, highs):
        raw_copy(distance).start()
    token_copy(0).start()
    tokens[tp_me] = mixed[tp_me]

    if pairs_count > 2:
        next_round(1)

    experts = lax.broadcasted_iota(jnp.int32, (128, tok_count), 0)
    earlier = lax.broadcasted_iota(jnp.int32, (tok_count, tok_count), 0)
    later = lax.broadcasted_iota(jnp.int32, (tok_count, tok_count), 1)
    before = jnp.where(earlier < later, 1.0, 0.0).astype(jnp.bfloat16)
    slots = lax.broadcasted_iota(jnp.int32, (slot_count, tok_count), 0).astype(jnp.float32)
    for distance in range(1, tp_count):
        route_copy(distance).wait_recv()
    for piece in range(tp_count):
        routes = routes_all[piece]
        named = [experts == routes[pick : pick + 1, :] for pick in range(top_count)]
        hits = named[0].astype(jnp.float32)
        for pick in range(1, top_count):
            hits = hits + named[pick].astype(jnp.float32)
        rank = jnp.dot(hits.astype(jnp.bfloat16), before, preferred_element_type=jnp.float32)
        for pick in range(top_count):
            start = step_of(routes[pick : pick + 1, :], me, sp_count) * cap
            spot = jnp.sum(jnp.where(named[pick], rank, 0.0), axis=0, keepdims=True)
            spot = spot + start.astype(jnp.float32)
            picked_at[piece, pick] = jnp.where(slots == spot, 1.0, 0.0).astype(jnp.bfloat16)

    def gain_of(own):
        gain = gain_ref[0:group_width]
        for piece in range(1, tp_count):
            columns = slice(piece * group_width, (piece + 1) * group_width)
            gain = jnp.where(own == piece, gain_ref[columns], gain)
        return gain.astype(jnp.float32)[None, :]

    table = ranked(sp_count)
    near = [step for step in range(sp_count) if table[step] < NEAR]

    def is_near(step):
        if isinstance(step, int):
            return step in near
        found = step == near[0]
        for index in near[1:]:
            found = found | (step == index)
        return found

    for distance in range(1, tp_count):
        square2_copy(distance).wait_recv()
    square = squares2[0, 0:1, :]
    for distance in range(1, tp_count):
        square = square + squares2[distance, 0:1, :]
    ffn_scale = lax.rsqrt(as_column(square) / width + NORM_EPS)
    normed2 = (after_f32 * ffn_scale * gain_of(tp_me)).astype(jnp.bfloat16)
    for index in range(2, pairs_count - 1):
        next_round(index)
    for piece in range(tp_count):
        dispatch = picked_at[piece, 0]
        for pick in range(1, top_count):
            dispatch = dispatch + picked_at[piece, pick]
        rows = jnp.dot(
            dispatch,
            normed2[piece * tok_count : (piece + 1) * tok_count],
            preferred_element_type=jnp.float32,
        )
        rows = rows.reshape(sp_count, cap, group_width).astype(jnp.bfloat16)
        send_ref[:, piece % LANES, piece // LANES] = rows

    def near_rows(piece):
        spans = [slice(step * cap, (step + 1) * cap) for step in near]
        parts = []
        for part in spans:
            rows = picked_at[piece, 0, part]
            for pick in range(1, top_count):
                rows = rows + picked_at[piece, pick, part]
            parts.append(rows.astype(jnp.float32))
        return jnp.concatenate(parts, axis=0).astype(jnp.bfloat16)

    def fill_near(distance):
        far_f32 = mixed_far[distance - 1].reshape(tok_rows, group_width).astype(jnp.float32)
        far_gain = gain_of(far_piece(distance))
        far_normed = (far_f32 * ffn_scale * far_gain).astype(jnp.bfloat16)
        for piece in range(tp_count):
            rows = jnp.dot(
                near_rows(piece),
                far_normed[piece * tok_count : (piece + 1) * tok_count],
                preferred_element_type=jnp.float32,
            )
            rows = rows.reshape(len(near), cap, group_width).astype(jnp.bfloat16)
            send_near[distance - 1, :, piece % LANES, piece // LANES] = rows

    def near_copy(step, distance):
        peer = peer_of(step, me, sp_count)
        there = step_of(me, peer, sp_count)
        return pltpu.make_async_remote_copy(
            src_ref=send_near.at[distance - 1, near.index(step)],
            dst_ref=arrived.at[there, :, :, :, columns_of(far_piece(distance))],
            send_sem=near_send.at[near.index(step), distance - 1],
            recv_sem=side_recv.at[there, distance - 1],
            device_id=sp_id(peer),
            device_id_type=MESH,
        )

    def first_copy(step):
        peer = peer_of(step, me, sp_count)
        return pltpu.make_async_remote_copy(
            src_ref=send_ref.at[step],
            dst_ref=arrived.at[step_of(me, peer, sp_count), :, :, :, columns_of(tp_me)],
            send_sem=first_send.at[step],
            recv_sem=first_recv.at[step_of(me, peer, sp_count)],
            device_id=sp_id(peer),
            device_id_type=MESH,
        )

    def first_arrival(step):
        return pltpu.make_async_remote_copy(
            src_ref=send_ref.at[step],
            dst_ref=arrived.at[step, :, :, :, columns_of(tp_me)],
            send_sem=first_send.at[step],
            recv_sem=first_recv.at[step],
            device_id=sp_id(peer_of(step, me, sp_count)),
            device_id_type=MESH,
        )

    def side_copy(step, distance):
        block = arrived.at[step, :, :, :, columns_of(tp_me)]
        return pltpu.make_async_remote_copy(
            src_ref=block,
            dst_ref=block,
            send_sem=side_send.at[step, distance - 1],
            recv_sem=side_recv.at[step, distance - 1],
            device_id=side_id(distance),
            device_id_type=MESH,
        )

    def pair_copy(step, distance):
        piece = from_high(distance) * LANES + low
        block = arrived.at[step, :, :, :, columns_of(piece)]
        return pltpu.make_async_remote_copy(
            src_ref=block,
            dst_ref=block,
            send_sem=pair_send.at[step, distance],
            recv_sem=pair_recv.at[step, distance],
            device_id=pair_id,
            device_id_type=MESH,
        )

    def steps_of(chunk):
        return [chunk * group + index for index in range(group)]

    def to_sides(step):
        for distance in range(1, highs):
            side_copy(step, distance).start()

    def share(step):
        if isinstance(step, int):
            if not is_near(step):
                to_sides(step)
        else:
            pl.when(jnp.logical_not(is_near(step)))(lambda: to_sides(step))
        pair_copy(step, 0).start()

    def spread(chunk):
        for step in steps_of(chunk):
            if not (isinstance(step, int) and step == 0):
                first_arrival(step).wait_recv()
            share(step)

    def pass_on(chunk):
        for step in steps_of(chunk):
            for distance in range(1, highs):
                if not (isinstance(step, int) and step == 0):
                    side_copy(step, distance).wait_recv()
                pair_copy(step, distance).start()

    def settle(chunk):
        for step in steps_of(chunk):
            for distance in range(highs):
                pair_copy(step, distance).wait_recv()

    def span(chunk):
        return pl.ds(chunk * group, group)

    tile = col_tile(ff_width)
    tiles = ff_width // tile
    out_tile = col_tile(width)

    def gate_up(chunk, first, last):
        rows = as_rows(arrived[span(chunk)])
        for index in range(first, last):
            columns = slice(index * tile, (index + 1) * tile)
            gate_val = jnp.dot(rows, gate[:, columns], preferred_element_type=jnp.float32)
            up_val = jnp.dot(rows, up[:, columns], preferred_element_type=jnp.float32)
            hidden[:, columns] = (jax.nn.silu(gate_val) * up_val).astype(jnp.bfloat16)

    def project(chunk):
        for index in range(width // out_tile):
            columns = slice(index * out_tile, (index + 1) * out_tile)
            block = jnp.dot(hidden[...], down[:, columns], preferred_element_type=jnp.float32)
            block = block.reshape(group, LANES, highs, cap, out_tile).astype(jnp.bfloat16)
            partial[span(chunk), :, :, :, columns] = block

    def back_pair_copy(chunk):
        return pltpu.make_async_remote_copy(
            src_ref=partial.at[span(chunk), other_low],
            dst_ref=pair_in.at[span(chunk)],
            send_sem=back_pair.at[0, chunk],
            recv_sem=back_pair.at[1, chunk],
            device_id=pair_id,
            device_id_type=MESH,
        )

    def back_side_copy(chunk, distance):
        return pltpu.make_async_remote_copy(
            src_ref=pair_sum.at[distance - 1, span(chunk)],
            dst_ref=side_in.at[distance - 1, span(chunk)],
            send_sem=back_side.at[0, chunk, distance - 1],
            recv_sem=back_side.at[1, chunk, distance - 1],
            device_id=side_id(distance),
            device_id_type=MESH,
        )

    def back_copy(step):
        peer = peer_of(step, me, sp_count)
        return pltpu.make_async_remote_copy(
            src_ref=served.at[step],
            dst_ref=returned.at[step_of(me, peer, sp_count)],
            send_sem=back_send.at[step],
            recv_sem=back_recv.at[step_of(me, peer, sp_count)],
            device_id=sp_id(peer),
            device_id_type=MESH,
        )

    def back_arrival(step):
        return pltpu.make_async_remote_copy(
            src_ref=served.at[step],
            dst_ref=returned.at[step],
            send_sem=back_send.at[step],
            recv_sem=back_recv.at[step],
            device_id=sp_id(peer_of(step, me, sp_count)),
            device_id_type=MESH,
        )

    def pair_add(chunk):
        back_pair_copy(chunk).wait_recv()
        for distance in range(1, highs):
            target = side_high(distance)
            for step in steps_of(chunk):
                total = partial[step, low, target].astype(jnp.float32)
                total = total + pair_in[step, target].astype(jnp.float32)
                pair_sum[distance - 1, step] = total.astype(jnp.bfloat16)
            back_side_copy(chunk, distance).start()

    def side_add(chunk):
        for distance in range(1, highs):
            back_side_copy(chunk, distance).wait_recv()
        for step in steps_of(chunk):
            total = partial[step, low, high].astype(jnp.float32)
            total = total + pair_in[step, high].astype(jnp.float32)
            for distance in range(1, highs):
                total = total + side_in[distance - 1, step].astype(jnp.float32)
            total = total.astype(jnp.bfloat16)

            def keep(step=step, total=total):
                returned[step] = total

            def give(step=step, total=total):
                served[step] = total
                back_copy(step).start()

            if isinstance(step, int):
                (keep if step == 0 else give)()
            else:
                pl.when(step == 0)(keep)
                pl.when(step > 0)(give)

    issue = ISSUE if sp_count == len(ORDER) else tuple(range(1, sp_count))
    for step in issue:
        first_copy(step).start()
    arrived[0, :, :, :, columns_of(tp_me)] = send_ref[0]
    if group == 1:
        spread(0)
    for distance in range(1, highs):
        raw_copy(distance).wait_recv()
        fill_near(distance)
        for step in issue:
            if step in near:
                near_copy(step, distance).start()
        arrived[0, :, :, :, columns_of(far_piece(distance))] = send_near[distance - 1, 0]
        token_copy(distance).start()
        tokens[far_piece(distance)] = mixed_far[distance - 1, tp_me]

    if group == 1:
        pass_on(0)
    for chunk in range(0 if group > 1 else 1, min(SPREAD_AHEAD, chunks)):
        spread(chunk)
    for chunk in range(0 if group > 1 else 1, min(PASS_AHEAD, chunks)):
        pass_on(chunk)
    for copy in weight_copies:
        copy.wait()
    early = (tiles + 1) // 2

    def turn(chunk, carry):
        settle(chunk)
        gate_up(chunk, 0, early)

        @pl.when(chunk >= 1)
        def _():
            pair_add(chunk - 1)

        @pl.when(chunk + SPREAD_AHEAD < chunks)
        def _():
            spread(chunk + SPREAD_AHEAD)

        gate_up(chunk, early, tiles)

        @pl.when(chunk + PASS_AHEAD < chunks)
        def _():
            pass_on(chunk + PASS_AHEAD)

        @pl.when(chunk >= SIDE_LAG)
        def _():
            side_add(chunk - SIDE_LAG)

        project(chunk)
        back_pair_copy(chunk).start()
        return carry

    lax.fori_loop(0, chunks, turn, 0)
    pair_add(chunks - 1)
    for chunk in range(max(0, chunks - SIDE_LAG), chunks):
        side_add(chunk)

    for distance in range(highs):
        token_copy(distance).wait_recv()
    for step in range(1, sp_count):
        back_arrival(step).wait_recv()
    rows = as_rows(returned[...])
    route_weights = [as_column(weight_ref[pick : pick + 1, :]) for pick in range(top_count)]
    for piece in range(tp_count):
        columns = slice(piece * group_width, (piece + 1) * group_width)
        total = tokens[piece].astype(jnp.float32)
        for pick in range(top_count):
            picked = lax.dot_general(
                picked_at[tp_me, pick],
                rows[:, columns],
                (((0,), (0,)), ((), ())),
                preferred_element_type=jnp.float32,
            )
            total = total + route_weights[pick] * picked
        out_ref[:, columns] = total.astype(jnp.bfloat16)

    @pl.when(me + 1 < sp_count)
    def _():
        halo_copy.wait_send()

    for distance in range(1, tp_count):
        square_copy(distance).wait_send()
        square2_copy(distance).wait_send()
        route_copy(distance).wait_send()
    for distance in range(highs):
        token_copy(distance).wait_send()
    for distance in range(1, highs):
        raw_copy(distance).wait_send()
        for step in near[1:]:
            near_copy(step, distance).wait_send()

    def finish(step, carry):
        @pl.when(jnp.logical_not(is_near(step)))
        def _():
            for distance in range(1, highs):
                side_copy(step, distance).wait_send()

        for distance in range(highs):
            pair_copy(step, distance).wait_send()
        return carry

    def finish_far(step, carry):
        first_copy(step).wait_send()
        back_copy(step).wait_send()
        return carry

    def finish_back(chunk, carry):
        back_pair_copy(chunk).wait_send()
        for distance in range(1, highs):
            back_side_copy(chunk, distance).wait_send()
        return carry

    lax.fori_loop(0, sp_count, finish, 0)
    lax.fori_loop(1, sp_count, finish_far, 0)
    lax.fori_loop(0, chunks, finish_back, 0)


def per_device(
    stream, mix_gain, pool_weight, pool_scale, ffn_gain, routes, route_weight, w_gate, w_up, w_down
):
    tok_rows, group_width = stream.shape
    tp_count = lax.axis_size("tp")
    sp_count = lax.axis_size("sp")
    width = group_width * tp_count
    tok_count, top_count = routes.shape
    cap = 2 * tok_count * top_count // sp_count
    halo_rows = 2 ** (pool_weight.shape[0] * tp_count)
    highs = tp_count // LANES
    chunks = chunk_count(sp_count)
    chunk_rows = sp_count // chunks * tp_count * cap
    ff_width = w_gate.shape[2]
    half = jnp.bfloat16
    vmem = pl.BlockSpec(memory_space=pltpu.VMEM)
    hbm = pl.BlockSpec(memory_space=pl.ANY)
    dma = pltpu.SemaphoreType.DMA
    rounds = max(1, sp_count // LANES - 1)
    return pl.pallas_call(
        functools.partial(expert_kernel, sp_count, tp_count, cap),
        out_shape=jax.ShapeDtypeStruct((tok_count, width), half),
        in_specs=[vmem] * 7 + [hbm] * 3,
        out_specs=vmem,
        scratch_shapes=[
            pltpu.VMEM((tp_count, 8, tok_rows), jnp.float32),
            pltpu.VMEM((tp_count, 8, tok_rows), jnp.float32),
            pltpu.VMEM((tp_count, top_count, tok_count), jnp.int32),
            pltpu.VMEM((halo_rows, group_width), half),
            pltpu.VMEM((halo_rows, group_width), half),
            pltpu.VMEM((tp_count, tok_count, group_width), half),
            pltpu.VMEM((highs - 1, tp_count, tok_count, group_width), half),
            pltpu.VMEM((tp_count, tok_count, group_width), half),
            pltpu.VMEM((tp_count, top_count, sp_count * cap, tok_count), half),
            pltpu.VMEM((sp_count, LANES, highs, cap, group_width), half),
            pltpu.VMEM((highs - 1, min(NEAR, sp_count), LANES, highs, cap, group_width), half),
            pltpu.VMEM(w_gate.shape[1:], half),
            pltpu.VMEM(w_up.shape[1:], half),
            pltpu.VMEM(w_down.shape[1:], half),
            pltpu.VMEM((sp_count, LANES, highs, cap, width), half),
            pltpu.VMEM((chunk_rows, ff_width), half),
            pltpu.VMEM((sp_count, LANES, highs, cap, width), half),
            pltpu.VMEM((sp_count, highs, cap, width), half),
            pltpu.VMEM((highs - 1, sp_count, cap, width), half),
            pltpu.VMEM((highs - 1, sp_count, cap, width), half),
            pltpu.VMEM((sp_count, cap, width), half),
            pltpu.VMEM((sp_count, cap, width), half),
            pltpu.SemaphoreType.REGULAR((rounds,)),
            dma((2, tp_count - 1)),
            dma((2, tp_count - 1)),
            dma((2, tp_count - 1)),
            dma((2,)),
            dma((2, highs - 1)),
            dma((2, highs)),
            dma((3,)),
            dma((sp_count,)),
            dma((sp_count,)),
            dma((min(NEAR, sp_count), highs - 1)),
            dma((sp_count, highs - 1)),
            dma((sp_count, highs - 1)),
            dma((sp_count, highs)),
            dma((sp_count, highs)),
            dma((2, chunks)),
            dma((2, chunks, highs - 1)),
            dma((sp_count,)),
            dma((sp_count,)),
        ],
        compiler_params=pltpu.CompilerParams(
            collective_id=1, has_side_effects=True, vmem_limit_bytes=60 * 1024 * 1024
        ),
    )(
        stream,
        mix_gain,
        pool_weight,
        pool_scale,
        ffn_gain,
        routes.T,
        route_weight.T,
        w_gate,
        w_up,
        w_down,
    )


def solution(mesh):
    in_specs = (
        P("sp", "tp"),
        P("tp"),
        P("tp", None, None),
        P("tp"),
        P(),
        P(("sp", "tp"), None),
        P(("sp", "tp"), None),
        P("sp", None, "tp"),
        P("sp", None, "tp"),
        P("sp", "tp", None),
    )
    out_specs = P(("sp", "tp"), None)
    return jax.shard_map(
        per_device, mesh=mesh, in_specs=in_specs, out_specs=out_specs, check_vma=False
    )
```

```python
import functools

import jax
import jax.numpy as jnp
from jax import lax
from jax.experimental import pallas as pl
from jax.experimental.pallas import tpu as pltpu
from jax.sharding import PartitionSpec as P

NORM_EPS = 1e-06


MESH = pl.DeviceIdType.MESH
COL_TILE = 256
LANES = 2
CHUNKS = 8
SPREAD_AHEAD = 4
PASS_AHEAD = 1
SIDE_LAG = 3
FIRST_SPREADS = 1
NEAR = 4
HALVES = 1
ORDER = (0, 7, 6, 3, 5, 2, 4, 1)
ISSUE = (1, 2, 4, 6, 3, 5, 7)


def as_rows(block):
    width = block.shape[-1]
    if block.shape[-2] % 16:
        return block.astype(jnp.float32).reshape(-1, width).astype(block.dtype)
    return block.reshape(-1, width)


def ranked(sp_count):
    if sp_count == len(ORDER):
        return ORDER
    return tuple(range(sp_count))


def looked_up(table, index):
    found = jnp.zeros_like(index)
    for key, value in enumerate(table):
        found = jnp.where(index == key, value, found)
    return found


def code_of(step, sp_count):
    table = ranked(sp_count)
    if isinstance(step, int):
        return jnp.int32(table[step])
    return looked_up(table, step)


def turned(me, code, sp_count):
    if sp_count != 4 * LANES:
        return code
    inside = ((me // LANES == 1) | (me // LANES == 2)) & (code >= sp_count // 2)
    return jnp.where(inside, code ^ LANES, code)


def step_of(peer, me, sp_count):
    table = ranked(sp_count)
    places = [table.index(code) for code in range(sp_count)]
    return looked_up(places, turned(me, peer ^ me, sp_count))


def peer_of(step, me, sp_count):
    return turned(me, code_of(step, sp_count), sp_count) ^ me


def as_column(row):
    size = row.shape[1]
    rows = lax.broadcasted_iota(jnp.int32, (size, size), 0)
    columns = lax.broadcasted_iota(jnp.int32, (size, size), 1)
    return jnp.sum(jnp.where(rows == columns, row, 0.0), axis=1, keepdims=True)


def as_row(column):
    size = column.shape[0]
    rows = lax.broadcasted_iota(jnp.int32, (size, size), 0)
    columns = lax.broadcasted_iota(jnp.int32, (size, size), 1)
    return jnp.sum(jnp.where(rows == columns, column, 0.0), axis=0, keepdims=True)


def chunk_count(sp_count):
    return CHUNKS if sp_count % CHUNKS == 0 else sp_count


def col_tile(width):
    return COL_TILE if width % COL_TILE == 0 else width


def expert_kernel(
    sp_count,
    tp_count,
    cap,
    stream_ref,
    mix_ref,
    pool_ref,
    scale_ref,
    gain_ref,
    routes_ref,
    weight_ref,
    gate_hbm,
    up_hbm,
    down_hbm,
    out_ref,
    squares,
    routes_all,
    tail,
    halo,
    mixed,
    mixed_far,
    tokens,
    picked_at,
    send_ref,
    send_near,
    gate,
    up,
    down,
    arrived,
    ready,
    hidden,
    partial,
    pair_in,
    pair_sum,
    side_in,
    served,
    returned,
    round_sem,
    square_sem,
    route_sem,
    halo_sem,
    raw_sem,
    token_sem,
    local_sem,
    first_send,
    first_recv,
    near_send,
    side_send,
    side_recv,
    pair_send,
    pair_recv,
    back_pair,
    back_side,
    back_send,
    back_recv,
):
    me = lax.axis_index("sp")
    tp_me = lax.axis_index("tp")
    high, low = tp_me // LANES, lax.rem(tp_me, LANES)
    highs = tp_count // LANES
    other_low = 1 - low
    pair_id = {"sp": me, "tp": high * LANES + other_low}
    pairs_count = sp_count // LANES
    chunks = chunk_count(sp_count)
    group = sp_count // chunks
    ff_width = gate.shape[1]
    tok_rows, group_width = stream_ref.shape
    width = group_width * tp_count
    halo_rows = halo.shape[0]
    tok_count = tokens.shape[1]
    top_count = routes_ref.shape[0]
    slot_count = sp_count * cap
    chunk_rows = hidden.shape[0]

    def side_high(distance):
        return lax.rem(high + distance, highs)

    def side_id(distance):
        return {"sp": me, "tp": side_high(distance) * LANES + low}

    def from_high(distance):
        return lax.rem(high - distance + highs, highs)

    def tp_id(distance):
        return {"sp": me, "tp": lax.rem(tp_me + distance, tp_count)}

    def sp_id(peer):
        return {"sp": peer, "tp": tp_me}

    def columns_of(piece):
        return pl.ds(pl.multiple_of(piece * group_width, group_width), group_width)

    weight_copies = [
        pltpu.make_async_copy(source.at[0], target, local_sem.at[index])
        for index, (source, target) in enumerate(((gate_hbm, gate), (up_hbm, up), (down_hbm, down)))
    ]
    for copy in weight_copies:
        copy.start()

    barrier = pltpu.get_barrier_semaphore()
    beside = me ^ 1
    across = jnp.where(lax.rem(me, LANES) == 1, me + 1, me - 1)
    has_across = (across >= 0) & (across < sp_count)
    has_up = me + LANES < sp_count
    has_down = me - LANES >= 0
    near_count = 1 + has_up.astype(jnp.int32) + has_down.astype(jnp.int32)

    def tell_near(sem):
        pl.semaphore_signal(sem, inc=1, device_id=sp_id(beside), device_id_type=MESH)

        @pl.when(has_up)
        def _():
            pl.semaphore_signal(sem, inc=1, device_id=sp_id(me + LANES), device_id_type=MESH)

        @pl.when(has_down)
        def _():
            pl.semaphore_signal(sem, inc=1, device_id=sp_id(me - LANES), device_id_type=MESH)

    for distance in range(1, tp_count):
        pl.semaphore_signal(barrier, inc=1, device_id=tp_id(distance), device_id_type=MESH)

    @pl.when(has_across)
    def _():
        pl.semaphore_signal(barrier, inc=1, device_id=sp_id(across), device_id_type=MESH)

    tell_near(barrier)

    def square_copy(distance):
        return pltpu.make_async_remote_copy(
            src_ref=squares.at[0],
            dst_ref=squares.at[distance],
            send_sem=square_sem.at[0, distance - 1],
            recv_sem=square_sem.at[1, distance - 1],
            device_id=tp_id(distance),
            device_id_type=MESH,
        )

    def route_copy(distance):
        return pltpu.make_async_remote_copy(
            src_ref=routes_ref,
            dst_ref=routes_all.at[tp_me],
            send_sem=route_sem.at[0, distance - 1],
            recv_sem=route_sem.at[1, distance - 1],
            device_id=tp_id(distance),
            device_id_type=MESH,
        )

    halo_copy = pltpu.make_async_remote_copy(
        src_ref=tail,
        dst_ref=halo,
        send_sem=halo_sem.at[0],
        recv_sem=halo_sem.at[1],
        device_id=sp_id(me + 1),
        device_id_type=MESH,
    )

    def far_piece(distance):
        return from_high(distance) * LANES + low

    def raw_copy(distance):
        return pltpu.make_async_remote_copy(
            src_ref=mixed,
            dst_ref=mixed_far.at[distance - 1],
            send_sem=raw_sem.at[0, distance - 1],
            recv_sem=raw_sem.at[1, distance - 1],
            device_id=side_id(distance),
            device_id_type=MESH,
        )

    def token_copy(distance):
        block = high * LANES + other_low
        source = mixed.at[block] if distance == 0 else mixed_far.at[distance - 1, block]
        return pltpu.make_async_remote_copy(
            src_ref=source,
            dst_ref=tokens.at[far_piece(distance)],
            send_sem=token_sem.at[0, distance],
            recv_sem=token_sem.at[1, distance],
            device_id=pair_id,
            device_id_type=MESH,
        )

    stream_f32 = stream_ref[...].astype(jnp.float32)
    own_square = as_row(jnp.sum(stream_f32 * stream_f32, axis=1, keepdims=True))
    squares[0] = jnp.broadcast_to(own_square, squares.shape[1:])
    pl.semaphore_wait(barrier, tp_count - 1 + near_count + has_across.astype(jnp.int32))
    for distance in range(1, tp_count):
        square_copy(distance).start()
    for distance in range(1, tp_count):
        route_copy(distance).start()
    if pairs_count > 1:
        tell_near(round_sem.at[0])
    routes_all[tp_me] = routes_ref[...]

    window_len = jnp.left_shift(jnp.int32(2), tp_me)
    first_row = me * tok_rows
    row_at = lax.broadcasted_iota(jnp.int32, (tok_rows, tok_rows), 0)
    source_at = lax.broadcasted_iota(jnp.int32, (tok_rows, tok_rows), 1)
    lag = row_at - source_at
    band = jnp.where((lag >= 0) & (lag < window_len), 1.0, 0.0).astype(jnp.bfloat16)
    row_at = lax.broadcasted_iota(jnp.int32, (halo_rows, halo_rows), 0)
    source_at = lax.broadcasted_iota(jnp.int32, (halo_rows, halo_rows), 1) - halo_rows
    reach = (row_at - source_at < window_len) & (first_row + source_at >= 0)
    halo_band = jnp.where(reach, 1.0, 0.0).astype(jnp.bfloat16)
    position = first_row + lax.broadcasted_iota(jnp.int32, (tok_rows, 1), 0)
    window_count = jnp.minimum(position + 1, window_len).astype(jnp.float32)
    pool_scale = scale_ref[...].astype(jnp.float32)[None, :]

    for distance in range(1, tp_count):
        square_copy(distance).wait_recv()
    square = squares[0, 0:1, :]
    for distance in range(1, tp_count):
        square = square + squares[distance, 0:1, :]
    row_scale = lax.rsqrt(as_column(square) / width + NORM_EPS)
    normed = stream_f32 * row_scale * mix_ref[...].astype(jnp.float32)[None, :]
    normed = normed.astype(jnp.bfloat16)
    tail[...] = normed[tok_rows - halo_rows :]

    @pl.when(me + 1 < sp_count)
    def _():
        halo_copy.start()

    def mix(sums, counts, own, rows):
        pooled = (sums / counts - own.astype(jnp.float32)).astype(jnp.bfloat16)
        mixer_out = jnp.dot(pooled, pool_ref[0], preferred_element_type=jnp.float32)
        return (rows + mixer_out * pool_scale).astype(jnp.bfloat16)

    window_sum = jnp.dot(band, normed, preferred_element_type=jnp.float32)
    after_mix = mix(window_sum, window_count, normed, stream_f32)
    for piece in range(tp_count):
        mixed[piece] = after_mix[piece * tok_count : (piece + 1) * tok_count]

    def next_round(index):
        pl.semaphore_wait(round_sem.at[index], near_count)
        if index + 2 < pairs_count:
            tell_near(round_sem.at[index + 1])

    experts = lax.broadcasted_iota(jnp.int32, (128, tok_count), 0)
    earlier = lax.broadcasted_iota(jnp.int32, (tok_count, tok_count), 0)
    later = lax.broadcasted_iota(jnp.int32, (tok_count, tok_count), 1)
    before = jnp.where(earlier < later, 1.0, 0.0).astype(jnp.bfloat16)
    slots = lax.broadcasted_iota(jnp.int32, (slot_count, tok_count), 0).astype(jnp.float32)
    for distance in range(1, tp_count):
        route_copy(distance).wait_recv()
    for piece in range(tp_count):
        routes = routes_all[piece]
        named = [experts == routes[pick : pick + 1, :] for pick in range(top_count)]
        hits = named[0].astype(jnp.float32)
        for pick in range(1, top_count):
            hits = hits + named[pick].astype(jnp.float32)
        rank = jnp.dot(hits.astype(jnp.bfloat16), before, preferred_element_type=jnp.float32)
        for pick in range(top_count):
            start = step_of(routes[pick : pick + 1, :], me, sp_count) * cap
            spot = jnp.sum(jnp.where(named[pick], rank, 0.0), axis=0, keepdims=True)
            spot = spot + start.astype(jnp.float32)
            picked_at[piece, pick] = jnp.where(slots == spot, 1.0, 0.0).astype(jnp.bfloat16)

    if pairs_count > 1:
        next_round(0)

    @pl.when(me > 0)
    def _():
        halo_copy.wait_recv()

    @pl.when(me == 0)
    def _():
        halo[...] = jnp.zeros_like(halo)

    first_sum = window_sum[:halo_rows]
    first_sum = first_sum + jnp.dot(halo_band, halo[...], preferred_element_type=jnp.float32)
    first_mix = mix(
        first_sum, window_count[:halo_rows], normed[:halo_rows], stream_f32[:halo_rows]
    )
    mixed[0, 0:halo_rows, :] = first_mix
    for distance in range(1, highs):
        raw_copy(distance).start()
    token_copy(0).start()
    tokens[tp_me] = mixed[tp_me]

    if pairs_count > 2:
        next_round(1)

    table = ranked(sp_count)
    near = [step for step in range(sp_count) if table[step] < NEAR]

    def is_near(step):
        if isinstance(step, int):
            return step in near
        found = step == near[0]
        for index in near[1:]:
            found = found | (step == index)
        return found

    for index in range(2, pairs_count - 1):
        next_round(index)
    for piece in range(tp_count):
        dispatch = picked_at[piece, 0]
        for pick in range(1, top_count):
            dispatch = dispatch + picked_at[piece, pick]
        rows = jnp.dot(
            dispatch,
            mixed[piece],
            preferred_element_type=jnp.float32,
        )
        rows = rows.reshape(sp_count, cap, group_width).astype(jnp.bfloat16)
        send_ref[:, piece % LANES, piece // LANES] = rows

    def near_rows(piece):
        spans = [slice(step * cap, (step + 1) * cap) for step in near]
        parts = []
        for part in spans:
            rows = picked_at[piece, 0, part]
            for pick in range(1, top_count):
                rows = rows + picked_at[piece, pick, part]
            parts.append(rows.astype(jnp.float32))
        return jnp.concatenate(parts, axis=0).astype(jnp.bfloat16)

    def fill_near(distance):
        for piece in range(tp_count):
            rows = jnp.dot(
                near_rows(piece),
                mixed_far[distance - 1, piece],
                preferred_element_type=jnp.float32,
            )
            rows = rows.reshape(len(near), cap, group_width).astype(jnp.bfloat16)
            send_near[distance - 1, :, piece % LANES, piece // LANES] = rows

    def near_copy(step, distance):
        peer = peer_of(step, me, sp_count)
        there = step_of(me, peer, sp_count)
        return pltpu.make_async_remote_copy(
            src_ref=send_near.at[distance - 1, near.index(step)],
            dst_ref=arrived.at[there, :, :, :, columns_of(far_piece(distance))],
            send_sem=near_send.at[near.index(step), distance - 1],
            recv_sem=side_recv.at[there, distance - 1],
            device_id=sp_id(peer),
            device_id_type=MESH,
        )

    def first_copy(step):
        peer = peer_of(step, me, sp_count)
        return pltpu.make_async_remote_copy(
            src_ref=send_ref.at[step],
            dst_ref=arrived.at[step_of(me, peer, sp_count), :, :, :, columns_of(tp_me)],
            send_sem=first_send.at[step],
            recv_sem=first_recv.at[step_of(me, peer, sp_count)],
            device_id=sp_id(peer),
            device_id_type=MESH,
        )

    def first_arrival(step):
        return pltpu.make_async_remote_copy(
            src_ref=send_ref.at[step],
            dst_ref=arrived.at[step, :, :, :, columns_of(tp_me)],
            send_sem=first_send.at[step],
            recv_sem=first_recv.at[step],
            device_id=sp_id(peer_of(step, me, sp_count)),
            device_id_type=MESH,
        )

    def side_copy(step, distance):
        block = arrived.at[step, :, :, :, columns_of(tp_me)]
        return pltpu.make_async_remote_copy(
            src_ref=block,
            dst_ref=block,
            send_sem=side_send.at[step, distance - 1],
            recv_sem=side_recv.at[step, distance - 1],
            device_id=side_id(distance),
            device_id_type=MESH,
        )

    def pair_copy(step, distance):
        piece = from_high(distance) * LANES + low
        block = arrived.at[step, :, :, :, columns_of(piece)]
        return pltpu.make_async_remote_copy(
            src_ref=block,
            dst_ref=block,
            send_sem=pair_send.at[step, distance],
            recv_sem=pair_recv.at[step, distance],
            device_id=pair_id,
            device_id_type=MESH,
        )

    def steps_of(chunk):
        return [chunk * group + index for index in range(group)]

    def to_sides(step):
        for distance in range(1, highs):
            side_copy(step, distance).start()

    def share(step):
        if isinstance(step, int):
            if not is_near(step):
                to_sides(step)
        else:
            pl.when(jnp.logical_not(is_near(step)))(lambda: to_sides(step))
        pair_copy(step, 0).start()

    def spread(chunk):
        for step in steps_of(chunk):
            if not (isinstance(step, int) and step == 0):
                first_arrival(step).wait_recv()
            share(step)

    def pass_on(chunk):
        for step in steps_of(chunk):
            for distance in range(1, highs):
                if not (isinstance(step, int) and step == 0):
                    side_copy(step, distance).wait_recv()
                pair_copy(step, distance).start()

    def settle(chunk):
        for step in steps_of(chunk):
            for distance in range(highs):
                pair_copy(step, distance).wait_recv()

    def span(chunk):
        return pl.ds(chunk * group, group)

    tile = col_tile(ff_width)
    tiles = ff_width // tile
    half_width = width // HALVES
    out_tile = col_tile(half_width)

    def prepare(chunk):
        square = jnp.zeros((chunk_rows, 1), jnp.float32)
        for piece in range(tp_count):
            columns = slice(piece * group_width, (piece + 1) * group_width)
            rows = as_rows(arrived[span(chunk), :, :, :, columns]).astype(jnp.float32)
            square = square + jnp.sum(rows * rows, axis=1, keepdims=True)
        ffn_scale = lax.rsqrt(square / width + NORM_EPS)
        for piece in range(tp_count):
            columns = slice(piece * group_width, (piece + 1) * group_width)
            rows = as_rows(arrived[span(chunk), :, :, :, columns]).astype(jnp.float32)
            gain = gain_ref[columns].astype(jnp.float32)[None, :]
            ready[:, columns] = (rows * ffn_scale * gain).astype(jnp.bfloat16)

    def gate_up(first, last):
        rows = ready[...]
        for index in range(first, last):
            columns = slice(index * tile, (index + 1) * tile)
            gate_val = jnp.dot(rows, gate[:, columns], preferred_element_type=jnp.float32)
            up_val = jnp.dot(rows, up[:, columns], preferred_element_type=jnp.float32)
            hidden[:, columns] = (jax.nn.silu(gate_val) * up_val).astype(jnp.bfloat16)

    def project(chunk, half):
        per_half = half_width // out_tile
        for index in range(half * per_half, (half + 1) * per_half):
            columns = slice(index * out_tile, (index + 1) * out_tile)
            block = jnp.dot(hidden[...], down[:, columns], preferred_element_type=jnp.float32)
            block = block.reshape(group, LANES, highs, cap, out_tile).astype(jnp.bfloat16)
            partial[span(chunk), :, :, :, columns] = block

    def part_of(half):
        return pl.ds(half * half_width, half_width)

    def back_pair_copy(chunk, half):
        return pltpu.make_async_remote_copy(
            src_ref=partial.at[span(chunk), other_low, :, :, part_of(half)],
            dst_ref=pair_in.at[span(chunk), :, :, part_of(half)],
            send_sem=back_pair.at[0, chunk, half],
            recv_sem=back_pair.at[1, chunk, half],
            device_id=pair_id,
            device_id_type=MESH,
        )

    def back_side_copy(chunk, half, distance):
        return pltpu.make_async_remote_copy(
            src_ref=pair_sum.at[distance - 1, span(chunk), :, part_of(half)],
            dst_ref=side_in.at[distance - 1, span(chunk), :, part_of(half)],
            send_sem=back_side.at[0, chunk, half, distance - 1],
            recv_sem=back_side.at[1, chunk, half, distance - 1],
            device_id=side_id(distance),
            device_id_type=MESH,
        )

    def back_copy(step, half):
        peer = peer_of(step, me, sp_count)
        there = step_of(me, peer, sp_count)
        return pltpu.make_async_remote_copy(
            src_ref=served.at[step, :, part_of(half)],
            dst_ref=returned.at[there, :, part_of(half)],
            send_sem=back_send.at[step, half],
            recv_sem=back_recv.at[there, half],
            device_id=sp_id(peer),
            device_id_type=MESH,
        )

    def back_arrival(step, half):
        return pltpu.make_async_remote_copy(
            src_ref=served.at[step, :, part_of(half)],
            dst_ref=returned.at[step, :, part_of(half)],
            send_sem=back_send.at[step, half],
            recv_sem=back_recv.at[step, half],
            device_id=sp_id(peer_of(step, me, sp_count)),
            device_id_type=MESH,
        )

    def pair_add(chunk, half):
        columns = part_of(half)
        back_pair_copy(chunk, half).wait_recv()
        for distance in range(1, highs):
            target = side_high(distance)
            for step in steps_of(chunk):
                total = partial[step, low, target, :, columns].astype(jnp.float32)
                total = total + pair_in[step, target, :, columns].astype(jnp.float32)
                pair_sum[distance - 1, step, :, columns] = total.astype(jnp.bfloat16)
            back_side_copy(chunk, half, distance).start()

    def side_add(chunk, half):
        columns = part_of(half)
        for distance in range(1, highs):
            back_side_copy(chunk, half, distance).wait_recv()
        for step in steps_of(chunk):
            total = partial[step, low, high, :, columns].astype(jnp.float32)
            total = total + pair_in[step, high, :, columns].astype(jnp.float32)
            for distance in range(1, highs):
                total = total + side_in[distance - 1, step, :, columns].astype(jnp.float32)
            total = total.astype(jnp.bfloat16)

            def keep(step=step, total=total):
                returned[step, :, columns] = total

            def give(step=step, total=total):
                served[step, :, columns] = total
                back_copy(step, half).start()

            if isinstance(step, int):
                (keep if step == 0 else give)()
            else:
                pl.when(step == 0)(keep)
                pl.when(step > 0)(give)

    issue = ISSUE if sp_count == len(ORDER) else tuple(range(1, sp_count))
    for step in issue:
        first_copy(step).start()
    arrived[0, :, :, :, columns_of(tp_me)] = send_ref[0]
    if group == 1:
        spread(0)
    for distance in range(1, highs):
        raw_copy(distance).wait_recv()
        fill_near(distance)
        for step in issue:
            if step in near:
                near_copy(step, distance).start()
        arrived[0, :, :, :, columns_of(far_piece(distance))] = send_near[distance - 1, 0]
        token_copy(distance).start()
        tokens[far_piece(distance)] = mixed_far[distance - 1, tp_me]

    if group > 1:
        spread(0)
    pass_on(0)
    for copy in weight_copies:
        copy.wait()
    early = (tiles + 1) // 2

    def finish_rows(chunk):
        for half in range(HALVES):
            project(chunk, half)
            back_pair_copy(chunk, half).start()

    settle(0)
    prepare(0)
    gate_up(0, tiles)
    for chunk in range(1, min(1 + FIRST_SPREADS, chunks)):
        spread(chunk)
    finish_rows(0)
    for chunk in range(1 + FIRST_SPREADS, min(SPREAD_AHEAD, chunks)):
        spread(chunk)
    for chunk in range(1, min(1 + PASS_AHEAD, chunks)):
        pass_on(chunk)

    def turn(chunk, carry):
        settle(chunk)
        prepare(chunk)
        gate_up(0, early)
        for half in range(HALVES):
            pair_add(chunk - 1, half)

        if SPREAD_AHEAD < chunks:

            @pl.when(chunk == 1)
            def _():
                spread(SPREAD_AHEAD)

        @pl.when(chunk + SPREAD_AHEAD < chunks)
        def _():
            spread(chunk + SPREAD_AHEAD)

        gate_up(early, tiles)

        @pl.when(chunk + PASS_AHEAD < chunks)
        def _():
            pass_on(chunk + PASS_AHEAD)

        @pl.when(chunk >= SIDE_LAG)
        def _():
            for half in range(HALVES):
                side_add(chunk - SIDE_LAG, half)

        finish_rows(chunk)
        return carry

    lax.fori_loop(1, chunks, turn, 0)
    last = chunks - 1
    for chunk in range(max(0, chunks - SIDE_LAG), last - 1):
        for half in range(HALVES):
            side_add(chunk, half)
    for half in range(HALVES):
        pair_add(last, half)
    for chunk in range(max(0, last - 1), chunks):
        for half in range(HALVES):
            side_add(chunk, half)

    for distance in range(highs):
        token_copy(distance).wait_recv()
    for step in range(1, sp_count):
        for half in range(HALVES):
            back_arrival(step, half).wait_recv()
    rows = as_rows(returned[...])
    route_weights = [as_column(weight_ref[pick : pick + 1, :]) for pick in range(top_count)]
    for piece in range(tp_count):
        columns = slice(piece * group_width, (piece + 1) * group_width)
        total = tokens[piece].astype(jnp.float32)
        for pick in range(top_count):
            picked = lax.dot_general(
                picked_at[tp_me, pick],
                rows[:, columns],
                (((0,), (0,)), ((), ())),
                preferred_element_type=jnp.float32,
            )
            total = total + route_weights[pick] * picked
        out_ref[:, columns] = total.astype(jnp.bfloat16)

    @pl.when(me + 1 < sp_count)
    def _():
        halo_copy.wait_send()

    for distance in range(1, tp_count):
        square_copy(distance).wait_send()
        route_copy(distance).wait_send()
    for distance in range(highs):
        token_copy(distance).wait_send()
    for distance in range(1, highs):
        raw_copy(distance).wait_send()
        for step in near[1:]:
            near_copy(step, distance).wait_send()

    def finish(step, carry):
        @pl.when(jnp.logical_not(is_near(step)))
        def _():
            for distance in range(1, highs):
                side_copy(step, distance).wait_send()

        for distance in range(highs):
            pair_copy(step, distance).wait_send()
        return carry

    def finish_far(step, carry):
        first_copy(step).wait_send()
        for half in range(HALVES):
            back_copy(step, half).wait_send()
        return carry

    def finish_back(chunk, carry):
        for half in range(HALVES):
            back_pair_copy(chunk, half).wait_send()
            for distance in range(1, highs):
                back_side_copy(chunk, half, distance).wait_send()
        return carry

    lax.fori_loop(0, sp_count, finish, 0)
    lax.fori_loop(1, sp_count, finish_far, 0)
    lax.fori_loop(0, chunks, finish_back, 0)


def per_device(
    stream, mix_gain, pool_weight, pool_scale, ffn_gain, routes, route_weight, w_gate, w_up, w_down
):
    tok_rows, group_width = stream.shape
    tp_count = lax.axis_size("tp")
    sp_count = lax.axis_size("sp")
    width = group_width * tp_count
    tok_count, top_count = routes.shape
    cap = 2 * tok_count * top_count // sp_count
    halo_rows = 2 ** (pool_weight.shape[0] * tp_count)
    highs = tp_count // LANES
    chunks = chunk_count(sp_count)
    chunk_rows = sp_count // chunks * tp_count * cap
    ff_width = w_gate.shape[2]
    half = jnp.bfloat16
    vmem = pl.BlockSpec(memory_space=pltpu.VMEM)
    hbm = pl.BlockSpec(memory_space=pl.ANY)
    dma = pltpu.SemaphoreType.DMA
    rounds = max(1, sp_count // LANES - 1)
    return pl.pallas_call(
        functools.partial(expert_kernel, sp_count, tp_count, cap),
        out_shape=jax.ShapeDtypeStruct((tok_count, width), half),
        in_specs=[vmem] * 7 + [hbm] * 3,
        out_specs=vmem,
        scratch_shapes=[
            pltpu.VMEM((tp_count, 8, tok_rows), jnp.float32),
            pltpu.VMEM((tp_count, top_count, tok_count), jnp.int32),
            pltpu.VMEM((halo_rows, group_width), half),
            pltpu.VMEM((halo_rows, group_width), half),
            pltpu.VMEM((tp_count, tok_count, group_width), half),
            pltpu.VMEM((highs - 1, tp_count, tok_count, group_width), half),
            pltpu.VMEM((tp_count, tok_count, group_width), half),
            pltpu.VMEM((tp_count, top_count, sp_count * cap, tok_count), half),
            pltpu.VMEM((sp_count, LANES, highs, cap, group_width), half),
            pltpu.VMEM((highs - 1, min(NEAR, sp_count), LANES, highs, cap, group_width), half),
            pltpu.VMEM(w_gate.shape[1:], half),
            pltpu.VMEM(w_up.shape[1:], half),
            pltpu.VMEM(w_down.shape[1:], half),
            pltpu.VMEM((sp_count, LANES, highs, cap, width), half),
            pltpu.VMEM((chunk_rows, width), half),
            pltpu.VMEM((chunk_rows, ff_width), half),
            pltpu.VMEM((sp_count, LANES, highs, cap, width), half),
            pltpu.VMEM((sp_count, highs, cap, width), half),
            pltpu.VMEM((highs - 1, sp_count, cap, width), half),
            pltpu.VMEM((highs - 1, sp_count, cap, width), half),
            pltpu.VMEM((sp_count, cap, width), half),
            pltpu.VMEM((sp_count, cap, width), half),
            pltpu.SemaphoreType.REGULAR((rounds,)),
            dma((2, tp_count - 1)),
            dma((2, tp_count - 1)),
            dma((2,)),
            dma((2, highs - 1)),
            dma((2, highs)),
            dma((3,)),
            dma((sp_count,)),
            dma((sp_count,)),
            dma((min(NEAR, sp_count), highs - 1)),
            dma((sp_count, highs - 1)),
            dma((sp_count, highs - 1)),
            dma((sp_count, highs)),
            dma((sp_count, highs)),
            dma((2, chunks, HALVES)),
            dma((2, chunks, HALVES, highs - 1)),
            dma((sp_count, HALVES)),
            dma((sp_count, HALVES)),
        ],
        compiler_params=pltpu.CompilerParams(
            collective_id=1, has_side_effects=True, vmem_limit_bytes=60 * 1024 * 1024
        ),
    )(
        stream,
        mix_gain,
        pool_weight,
        pool_scale,
        ffn_gain,
        routes.T,
        route_weight.T,
        w_gate,
        w_up,
        w_down,
    )


def solution(mesh):
    in_specs = (
        P("sp", "tp"),
        P("tp"),
        P("tp", None, None),
        P("tp"),
        P(),
        P(("sp", "tp"), None),
        P(("sp", "tp"), None),
        P("sp", None, "tp"),
        P("sp", None, "tp"),
        P("sp", "tp", None),
    )
    out_specs = P(("sp", "tp"), None)
    return jax.shard_map(
        per_device, mesh=mesh, in_specs=in_specs, out_specs=out_specs, check_vma=False
    )
```

```python
import functools

import jax
import jax.numpy as jnp
from jax import lax
from jax.experimental import pallas as pl
from jax.experimental.pallas import tpu as pltpu
from jax.sharding import PartitionSpec as P

NORM_EPS = 1e-06


MESH = pl.DeviceIdType.MESH
COL_TILE = 256
LANES = 2
CHUNKS = 8
SPREAD_AHEAD = 4
PASS_AHEAD = 1
SIDE_LAG = 3
FIRST_SPREADS = 1
NEAR = 4
HALVES = 1
ORDER = (0, 7, 6, 3, 5, 2, 4, 1)
ISSUE = (1, 2, 4, 6, 3, 5, 7)


def as_rows(block):
    width = block.shape[-1]
    if block.shape[-2] % 16:
        return block.astype(jnp.float32).reshape(-1, width).astype(block.dtype)
    return block.reshape(-1, width)


def ranked(sp_count):
    if sp_count == len(ORDER):
        return ORDER
    return tuple(range(sp_count))


def looked_up(table, index):
    found = jnp.zeros_like(index)
    for key, value in enumerate(table):
        found = jnp.where(index == key, value, found)
    return found


def code_of(step, sp_count):
    table = ranked(sp_count)
    if isinstance(step, int):
        return jnp.int32(table[step])
    return looked_up(table, step)


def turned(me, code, sp_count):
    if sp_count != 4 * LANES:
        return code
    inside = ((me // LANES == 1) | (me // LANES == 2)) & (code >= sp_count // 2)
    return jnp.where(inside, code ^ LANES, code)


def step_of(peer, me, sp_count):
    table = ranked(sp_count)
    places = [table.index(code) for code in range(sp_count)]
    return looked_up(places, turned(me, peer ^ me, sp_count))


def peer_of(step, me, sp_count):
    return turned(me, code_of(step, sp_count), sp_count) ^ me


def as_column(row):
    size = row.shape[1]
    rows = lax.broadcasted_iota(jnp.int32, (size, size), 0)
    columns = lax.broadcasted_iota(jnp.int32, (size, size), 1)
    return jnp.sum(jnp.where(rows == columns, row, 0.0), axis=1, keepdims=True)


def as_row(column):
    size = column.shape[0]
    rows = lax.broadcasted_iota(jnp.int32, (size, size), 0)
    columns = lax.broadcasted_iota(jnp.int32, (size, size), 1)
    return jnp.sum(jnp.where(rows == columns, column, 0.0), axis=0, keepdims=True)


def chunk_count(sp_count):
    return CHUNKS if sp_count % CHUNKS == 0 else sp_count


def col_tile(width):
    return COL_TILE if width % COL_TILE == 0 else width


def expert_kernel(
    sp_count,
    tp_count,
    cap,
    stream_ref,
    mix_ref,
    pool_ref,
    scale_ref,
    gain_ref,
    routes_ref,
    weight_ref,
    gate_hbm,
    up_hbm,
    down_hbm,
    out_ref,
    squares,
    routes_all,
    tail,
    halo,
    mixed,
    mixed_far,
    tokens,
    picked_at,
    send_ref,
    send_near,
    gate,
    up,
    down,
    arrived,
    ready,
    hidden,
    partial,
    pair_in,
    pair_sum,
    side_in,
    served,
    returned,
    summed,
    round_sem,
    square_sem,
    route_sem,
    halo_sem,
    raw_sem,
    token_sem,
    local_sem,
    first_send,
    first_recv,
    near_send,
    side_send,
    side_recv,
    pair_send,
    pair_recv,
    back_pair,
    back_side,
    back_send,
    back_recv,
):
    me = lax.axis_index("sp")
    tp_me = lax.axis_index("tp")
    high, low = tp_me // LANES, lax.rem(tp_me, LANES)
    highs = tp_count // LANES
    other_low = 1 - low
    pair_id = {"sp": me, "tp": high * LANES + other_low}
    pairs_count = sp_count // LANES
    chunks = chunk_count(sp_count)
    group = sp_count // chunks
    ff_width = gate.shape[1]
    tok_rows, group_width = stream_ref.shape
    width = group_width * tp_count
    halo_rows = halo.shape[0]
    tok_count = tokens.shape[1]
    top_count = routes_ref.shape[0]
    slot_count = sp_count * cap
    chunk_rows = hidden.shape[0]

    def side_high(distance):
        return lax.rem(high + distance, highs)

    def side_id(distance):
        return {"sp": me, "tp": side_high(distance) * LANES + low}

    def from_high(distance):
        return lax.rem(high - distance + highs, highs)

    def tp_id(distance):
        return {"sp": me, "tp": lax.rem(tp_me + distance, tp_count)}

    def sp_id(peer):
        return {"sp": peer, "tp": tp_me}

    def columns_of(piece):
        return pl.ds(pl.multiple_of(piece * group_width, group_width), group_width)

    weight_copies = [
        pltpu.make_async_copy(source.at[0], target, local_sem.at[index])
        for index, (source, target) in enumerate(((gate_hbm, gate), (up_hbm, up), (down_hbm, down)))
    ]
    for copy in weight_copies:
        copy.start()

    barrier = pltpu.get_barrier_semaphore()
    beside = me ^ 1
    across = jnp.where(lax.rem(me, LANES) == 1, me + 1, me - 1)
    has_across = (across >= 0) & (across < sp_count)
    has_up = me + LANES < sp_count
    has_down = me - LANES >= 0
    near_count = 1 + has_up.astype(jnp.int32) + has_down.astype(jnp.int32)

    def tell_near(sem):
        pl.semaphore_signal(sem, inc=1, device_id=sp_id(beside), device_id_type=MESH)

        @pl.when(has_up)
        def _():
            pl.semaphore_signal(sem, inc=1, device_id=sp_id(me + LANES), device_id_type=MESH)

        @pl.when(has_down)
        def _():
            pl.semaphore_signal(sem, inc=1, device_id=sp_id(me - LANES), device_id_type=MESH)

    for distance in range(1, tp_count):
        pl.semaphore_signal(barrier, inc=1, device_id=tp_id(distance), device_id_type=MESH)

    @pl.when(has_across)
    def _():
        pl.semaphore_signal(barrier, inc=1, device_id=sp_id(across), device_id_type=MESH)

    tell_near(barrier)

    def square_copy(distance):
        return pltpu.make_async_remote_copy(
            src_ref=squares.at[0],
            dst_ref=squares.at[distance],
            send_sem=square_sem.at[0, distance - 1],
            recv_sem=square_sem.at[1, distance - 1],
            device_id=tp_id(distance),
            device_id_type=MESH,
        )

    def route_copy(distance):
        return pltpu.make_async_remote_copy(
            src_ref=routes_ref,
            dst_ref=routes_all.at[tp_me],
            send_sem=route_sem.at[0, distance - 1],
            recv_sem=route_sem.at[1, distance - 1],
            device_id=tp_id(distance),
            device_id_type=MESH,
        )

    halo_copy = pltpu.make_async_remote_copy(
        src_ref=tail,
        dst_ref=halo,
        send_sem=halo_sem.at[0],
        recv_sem=halo_sem.at[1],
        device_id=sp_id(me + 1),
        device_id_type=MESH,
    )

    def far_piece(distance):
        return from_high(distance) * LANES + low

    def raw_copy(distance):
        return pltpu.make_async_remote_copy(
            src_ref=mixed,
            dst_ref=mixed_far.at[distance - 1],
            send_sem=raw_sem.at[0, distance - 1],
            recv_sem=raw_sem.at[1, distance - 1],
            device_id=side_id(distance),
            device_id_type=MESH,
        )

    def token_copy(distance):
        block = high * LANES + other_low
        source = mixed.at[block] if distance == 0 else mixed_far.at[distance - 1, block]
        return pltpu.make_async_remote_copy(
            src_ref=source,
            dst_ref=tokens.at[far_piece(distance)],
            send_sem=token_sem.at[0, distance],
            recv_sem=token_sem.at[1, distance],
            device_id=pair_id,
            device_id_type=MESH,
        )

    stream_f32 = stream_ref[...].astype(jnp.float32)
    own_square = as_row(jnp.sum(stream_f32 * stream_f32, axis=1, keepdims=True))
    squares[0] = jnp.broadcast_to(own_square, squares.shape[1:])
    pl.semaphore_wait(barrier, tp_count - 1 + near_count + has_across.astype(jnp.int32))
    for distance in range(1, tp_count):
        square_copy(distance).start()
    for distance in range(1, tp_count):
        route_copy(distance).start()
    if pairs_count > 1:
        tell_near(round_sem.at[0])
    routes_all[tp_me] = routes_ref[...]

    window_len = jnp.left_shift(jnp.int32(2), tp_me)
    first_row = me * tok_rows
    row_at = lax.broadcasted_iota(jnp.int32, (tok_rows, tok_rows), 0)
    source_at = lax.broadcasted_iota(jnp.int32, (tok_rows, tok_rows), 1)
    lag = row_at - source_at
    band = jnp.where((lag >= 0) & (lag < window_len), 1.0, 0.0).astype(jnp.bfloat16)
    row_at = lax.broadcasted_iota(jnp.int32, (halo_rows, halo_rows), 0)
    source_at = lax.broadcasted_iota(jnp.int32, (halo_rows, halo_rows), 1) - halo_rows
    reach = (row_at - source_at < window_len) & (first_row + source_at >= 0)
    halo_band = jnp.where(reach, 1.0, 0.0).astype(jnp.bfloat16)
    position = first_row + lax.broadcasted_iota(jnp.int32, (tok_rows, 1), 0)
    window_count = jnp.minimum(position + 1, window_len).astype(jnp.float32)
    pool_scale = scale_ref[...].astype(jnp.float32)[None, :]

    for distance in range(1, tp_count):
        square_copy(distance).wait_recv()
    square = squares[0, 0:1, :]
    for distance in range(1, tp_count):
        square = square + squares[distance, 0:1, :]
    row_scale = lax.rsqrt(as_column(square) / width + NORM_EPS)
    normed = stream_f32 * row_scale * mix_ref[...].astype(jnp.float32)[None, :]
    normed = normed.astype(jnp.bfloat16)
    tail[...] = normed[tok_rows - halo_rows :]

    @pl.when(me + 1 < sp_count)
    def _():
        halo_copy.start()

    def mix(sums, counts, own, rows):
        pooled = (sums / counts - own.astype(jnp.float32)).astype(jnp.bfloat16)
        mixer_out = jnp.dot(pooled, pool_ref[0], preferred_element_type=jnp.float32)
        return (rows + mixer_out * pool_scale).astype(jnp.bfloat16)

    window_sum = jnp.dot(band, normed, preferred_element_type=jnp.float32)
    after_mix = mix(window_sum, window_count, normed, stream_f32)
    for piece in range(tp_count):
        mixed[piece] = after_mix[piece * tok_count : (piece + 1) * tok_count]

    def next_round(index):
        pl.semaphore_wait(round_sem.at[index], near_count)
        if index + 2 < pairs_count:
            tell_near(round_sem.at[index + 1])

    experts = lax.broadcasted_iota(jnp.int32, (128, tok_count), 0)
    earlier = lax.broadcasted_iota(jnp.int32, (tok_count, tok_count), 0)
    later = lax.broadcasted_iota(jnp.int32, (tok_count, tok_count), 1)
    before = jnp.where(earlier < later, 1.0, 0.0).astype(jnp.bfloat16)
    slots = lax.broadcasted_iota(jnp.int32, (slot_count, tok_count), 0).astype(jnp.float32)
    for distance in range(1, tp_count):
        route_copy(distance).wait_recv()
    for piece in range(tp_count):
        routes = routes_all[piece]
        named = [experts == routes[pick : pick + 1, :] for pick in range(top_count)]
        hits = named[0].astype(jnp.float32)
        for pick in range(1, top_count):
            hits = hits + named[pick].astype(jnp.float32)
        rank = jnp.dot(hits.astype(jnp.bfloat16), before, preferred_element_type=jnp.float32)
        for pick in range(top_count):
            start = step_of(routes[pick : pick + 1, :], me, sp_count) * cap
            spot = jnp.sum(jnp.where(named[pick], rank, 0.0), axis=0, keepdims=True)
            spot = spot + start.astype(jnp.float32)
            picked_at[piece, pick] = jnp.where(slots == spot, 1.0, 0.0).astype(jnp.bfloat16)

    if pairs_count > 1:
        next_round(0)

    @pl.when(me > 0)
    def _():
        halo_copy.wait_recv()

    @pl.when(me == 0)
    def _():
        halo[...] = jnp.zeros_like(halo)

    first_sum = window_sum[:halo_rows]
    first_sum = first_sum + jnp.dot(halo_band, halo[...], preferred_element_type=jnp.float32)
    first_mix = mix(
        first_sum, window_count[:halo_rows], normed[:halo_rows], stream_f32[:halo_rows]
    )
    mixed[0, 0:halo_rows, :] = first_mix
    for distance in range(1, highs):
        raw_copy(distance).start()
    token_copy(0).start()
    tokens[tp_me] = mixed[tp_me]

    if pairs_count > 2:
        next_round(1)

    table = ranked(sp_count)
    near = [step for step in range(sp_count) if table[step] < NEAR]

    def is_near(step):
        if isinstance(step, int):
            return step in near
        found = step == near[0]
        for index in near[1:]:
            found = found | (step == index)
        return found

    for index in range(2, pairs_count - 1):
        next_round(index)
    for piece in range(tp_count):
        dispatch = picked_at[piece, 0]
        for pick in range(1, top_count):
            dispatch = dispatch + picked_at[piece, pick]
        rows = jnp.dot(
            dispatch,
            mixed[piece],
            preferred_element_type=jnp.float32,
        )
        rows = rows.reshape(sp_count, cap, group_width).astype(jnp.bfloat16)
        send_ref[:, piece % LANES, piece // LANES] = rows

    def near_rows(piece):
        spans = [slice(step * cap, (step + 1) * cap) for step in near]
        parts = []
        for part in spans:
            rows = picked_at[piece, 0, part]
            for pick in range(1, top_count):
                rows = rows + picked_at[piece, pick, part]
            parts.append(rows.astype(jnp.float32))
        return jnp.concatenate(parts, axis=0).astype(jnp.bfloat16)

    def fill_near(distance):
        for piece in range(tp_count):
            rows = jnp.dot(
                near_rows(piece),
                mixed_far[distance - 1, piece],
                preferred_element_type=jnp.float32,
            )
            rows = rows.reshape(len(near), cap, group_width).astype(jnp.bfloat16)
            send_near[distance - 1, :, piece % LANES, piece // LANES] = rows

    def near_copy(step, distance):
        peer = peer_of(step, me, sp_count)
        there = step_of(me, peer, sp_count)
        return pltpu.make_async_remote_copy(
            src_ref=send_near.at[distance - 1, near.index(step)],
            dst_ref=arrived.at[there, :, :, :, columns_of(far_piece(distance))],
            send_sem=near_send.at[near.index(step), distance - 1],
            recv_sem=side_recv.at[there, distance - 1],
            device_id=sp_id(peer),
            device_id_type=MESH,
        )

    def first_copy(step):
        peer = peer_of(step, me, sp_count)
        return pltpu.make_async_remote_copy(
            src_ref=send_ref.at[step],
            dst_ref=arrived.at[step_of(me, peer, sp_count), :, :, :, columns_of(tp_me)],
            send_sem=first_send.at[step],
            recv_sem=first_recv.at[step_of(me, peer, sp_count)],
            device_id=sp_id(peer),
            device_id_type=MESH,
        )

    def first_arrival(step):
        return pltpu.make_async_remote_copy(
            src_ref=send_ref.at[step],
            dst_ref=arrived.at[step, :, :, :, columns_of(tp_me)],
            send_sem=first_send.at[step],
            recv_sem=first_recv.at[step],
            device_id=sp_id(peer_of(step, me, sp_count)),
            device_id_type=MESH,
        )

    def side_copy(step, distance):
        block = arrived.at[step, :, :, :, columns_of(tp_me)]
        return pltpu.make_async_remote_copy(
            src_ref=block,
            dst_ref=block,
            send_sem=side_send.at[step, distance - 1],
            recv_sem=side_recv.at[step, distance - 1],
            device_id=side_id(distance),
            device_id_type=MESH,
        )

    def pair_copy(step, distance):
        piece = from_high(distance) * LANES + low
        block = arrived.at[step, :, :, :, columns_of(piece)]
        return pltpu.make_async_remote_copy(
            src_ref=block,
            dst_ref=block,
            send_sem=pair_send.at[step, distance],
            recv_sem=pair_recv.at[step, distance],
            device_id=pair_id,
            device_id_type=MESH,
        )

    def steps_of(chunk):
        return [chunk * group + index for index in range(group)]

    def to_sides(step):
        for distance in range(1, highs):
            side_copy(step, distance).start()

    def share(step):
        if isinstance(step, int):
            if not is_near(step):
                to_sides(step)
        else:
            pl.when(jnp.logical_not(is_near(step)))(lambda: to_sides(step))
        pair_copy(step, 0).start()

    def spread(chunk):
        for step in steps_of(chunk):
            if not (isinstance(step, int) and step == 0):
                first_arrival(step).wait_recv()
            share(step)

    def pass_on(chunk):
        for step in steps_of(chunk):
            for distance in range(1, highs):
                if not (isinstance(step, int) and step == 0):
                    side_copy(step, distance).wait_recv()
                pair_copy(step, distance).start()

    def settle(chunk):
        for step in steps_of(chunk):
            for distance in range(highs):
                pair_copy(step, distance).wait_recv()

    def span(chunk):
        return pl.ds(chunk * group, group)

    tile = col_tile(ff_width)
    tiles = ff_width // tile
    half_width = width // HALVES
    out_tile = col_tile(half_width)

    def prepare(chunk):
        square = jnp.zeros((chunk_rows, 1), jnp.float32)
        for piece in range(tp_count):
            columns = slice(piece * group_width, (piece + 1) * group_width)
            rows = as_rows(arrived[span(chunk), :, :, :, columns]).astype(jnp.float32)
            square = square + jnp.sum(rows * rows, axis=1, keepdims=True)
        ffn_scale = lax.rsqrt(square / width + NORM_EPS)
        for piece in range(tp_count):
            columns = slice(piece * group_width, (piece + 1) * group_width)
            rows = as_rows(arrived[span(chunk), :, :, :, columns]).astype(jnp.float32)
            gain = gain_ref[columns].astype(jnp.float32)[None, :]
            ready[:, columns] = (rows * ffn_scale * gain).astype(jnp.bfloat16)

    def gate_up(first, last):
        rows = ready[...]
        for index in range(first, last):
            columns = slice(index * tile, (index + 1) * tile)
            gate_val = jnp.dot(rows, gate[:, columns], preferred_element_type=jnp.float32)
            up_val = jnp.dot(rows, up[:, columns], preferred_element_type=jnp.float32)
            hidden[:, columns] = (jax.nn.silu(gate_val) * up_val).astype(jnp.bfloat16)

    def project(chunk, half):
        per_half = half_width // out_tile
        for index in range(half * per_half, (half + 1) * per_half):
            columns = slice(index * out_tile, (index + 1) * out_tile)
            block = jnp.dot(hidden[...], down[:, columns], preferred_element_type=jnp.float32)
            block = block.reshape(group, LANES, highs, cap, out_tile).astype(jnp.bfloat16)
            partial[span(chunk), :, :, :, columns] = block

    def part_of(half):
        return pl.ds(half * half_width, half_width)

    def back_pair_copy(chunk, half):
        return pltpu.make_async_remote_copy(
            src_ref=partial.at[span(chunk), other_low, :, :, part_of(half)],
            dst_ref=pair_in.at[span(chunk), :, :, part_of(half)],
            send_sem=back_pair.at[0, chunk, half],
            recv_sem=back_pair.at[1, chunk, half],
            device_id=pair_id,
            device_id_type=MESH,
        )

    def back_side_copy(chunk, half, distance):
        return pltpu.make_async_remote_copy(
            src_ref=pair_sum.at[distance - 1, span(chunk), :, part_of(half)],
            dst_ref=side_in.at[distance - 1, span(chunk), :, part_of(half)],
            send_sem=back_side.at[0, chunk, half, distance - 1],
            recv_sem=back_side.at[1, chunk, half, distance - 1],
            device_id=side_id(distance),
            device_id_type=MESH,
        )

    def back_copy(step, half):
        peer = peer_of(step, me, sp_count)
        there = step_of(me, peer, sp_count)
        return pltpu.make_async_remote_copy(
            src_ref=served.at[step, :, part_of(half)],
            dst_ref=returned.at[there, :, part_of(half)],
            send_sem=back_send.at[step, half],
            recv_sem=back_recv.at[there, half],
            device_id=sp_id(peer),
            device_id_type=MESH,
        )

    def back_arrival(step, half):
        return pltpu.make_async_remote_copy(
            src_ref=served.at[step, :, part_of(half)],
            dst_ref=returned.at[step, :, part_of(half)],
            send_sem=back_send.at[step, half],
            recv_sem=back_recv.at[step, half],
            device_id=sp_id(peer_of(step, me, sp_count)),
            device_id_type=MESH,
        )

    def pair_add(chunk, half):
        columns = part_of(half)
        back_pair_copy(chunk, half).wait_recv()
        for distance in range(1, highs):
            target = side_high(distance)
            for step in steps_of(chunk):
                total = partial[step, low, target, :, columns].astype(jnp.float32)
                total = total + pair_in[step, target, :, columns].astype(jnp.float32)
                pair_sum[distance - 1, step, :, columns] = total.astype(jnp.bfloat16)
            back_side_copy(chunk, half, distance).start()

    def side_add(chunk, half):
        columns = part_of(half)
        for distance in range(1, highs):
            back_side_copy(chunk, half, distance).wait_recv()
        for step in steps_of(chunk):
            total = partial[step, low, high, :, columns].astype(jnp.float32)
            total = total + pair_in[step, high, :, columns].astype(jnp.float32)
            for distance in range(1, highs):
                total = total + side_in[distance - 1, step, :, columns].astype(jnp.float32)
            total = total.astype(jnp.bfloat16)

            def keep(step=step, total=total):
                returned[step, :, columns] = total

            def give(step=step, total=total):
                served[step, :, columns] = total
                back_copy(step, half).start()

            if isinstance(step, int):
                (keep if step == 0 else give)()
            else:
                pl.when(step == 0)(keep)
                pl.when(step > 0)(give)

    issue = ISSUE if sp_count == len(ORDER) else tuple(range(1, sp_count))
    for step in issue:
        first_copy(step).start()
    arrived[0, :, :, :, columns_of(tp_me)] = send_ref[0]
    if group == 1:
        spread(0)
    for distance in range(1, highs):
        raw_copy(distance).wait_recv()
        fill_near(distance)
        for step in issue:
            if step in near:
                near_copy(step, distance).start()
        arrived[0, :, :, :, columns_of(far_piece(distance))] = send_near[distance - 1, 0]
        token_copy(distance).start()
        tokens[far_piece(distance)] = mixed_far[distance - 1, tp_me]

    if group > 1:
        spread(0)
    pass_on(0)
    for copy in weight_copies:
        copy.wait()
    early = (tiles + 1) // 2

    def finish_rows(chunk):
        for half in range(HALVES):
            project(chunk, half)
            back_pair_copy(chunk, half).start()

    settle(0)
    prepare(0)
    gate_up(0, tiles)
    for chunk in range(1, min(1 + FIRST_SPREADS, chunks)):
        spread(chunk)
    finish_rows(0)
    for chunk in range(1 + FIRST_SPREADS, min(SPREAD_AHEAD, chunks)):
        spread(chunk)
    for chunk in range(1, min(1 + PASS_AHEAD, chunks)):
        pass_on(chunk)

    def turn(chunk, carry):
        settle(chunk)
        prepare(chunk)
        gate_up(0, early)
        for half in range(HALVES):
            pair_add(chunk - 1, half)

        if SPREAD_AHEAD < chunks:

            @pl.when(chunk == 1)
            def _():
                spread(SPREAD_AHEAD)

        @pl.when(chunk + SPREAD_AHEAD < chunks)
        def _():
            spread(chunk + SPREAD_AHEAD)

        gate_up(early, tiles)

        @pl.when(chunk + PASS_AHEAD < chunks)
        def _():
            pass_on(chunk + PASS_AHEAD)

        @pl.when(chunk >= SIDE_LAG)
        def _():
            for half in range(HALVES):
                side_add(chunk - SIDE_LAG, half)

        finish_rows(chunk)
        return carry

    lax.fori_loop(1, chunks, turn, 0)
    last = chunks - 1
    for chunk in range(max(0, chunks - SIDE_LAG), last - 1):
        for half in range(HALVES):
            side_add(chunk, half)
    for half in range(HALVES):
        pair_add(last, half)
    for chunk in range(max(0, last - 1), chunks):
        for half in range(HALVES):
            side_add(chunk, half)

    for distance in range(highs):
        token_copy(distance).wait_recv()
    route_weights = [as_column(weight_ref[pick : pick + 1, :]) for pick in range(top_count)]

    def gather(first, last):
        for step in range(max(1, first), last):
            for half in range(HALVES):
                back_arrival(step, half).wait_recv()
        rows = as_rows(returned[first:last])
        for piece in range(tp_count):
            columns = slice(piece * group_width, (piece + 1) * group_width)
            total = tokens[piece].astype(jnp.float32) if first == 0 else summed[:, columns]
            for pick in range(top_count):
                picked = lax.dot_general(
                    picked_at[tp_me, pick, first * cap : last * cap],
                    rows[:, columns],
                    (((0,), (0,)), ((), ())),
                    preferred_element_type=jnp.float32,
                )
                total = total + route_weights[pick] * picked
            if last == sp_count:
                out_ref[:, columns] = total.astype(jnp.bfloat16)
            else:
                summed[:, columns] = total

    middle = sp_count * 5 // 8
    if middle:
        gather(0, middle)
    gather(middle, sp_count)

    @pl.when(me + 1 < sp_count)
    def _():
        halo_copy.wait_send()

    for distance in range(1, tp_count):
        square_copy(distance).wait_send()
        route_copy(distance).wait_send()
    for distance in range(highs):
        token_copy(distance).wait_send()
    for distance in range(1, highs):
        raw_copy(distance).wait_send()
        for step in near[1:]:
            near_copy(step, distance).wait_send()

    def finish(step, carry):
        @pl.when(jnp.logical_not(is_near(step)))
        def _():
            for distance in range(1, highs):
                side_copy(step, distance).wait_send()

        for distance in range(highs):
            pair_copy(step, distance).wait_send()
        return carry

    def finish_far(step, carry):
        first_copy(step).wait_send()
        for half in range(HALVES):
            back_copy(step, half).wait_send()
        return carry

    def finish_back(chunk, carry):
        for half in range(HALVES):
            back_pair_copy(chunk, half).wait_send()
            for distance in range(1, highs):
                back_side_copy(chunk, half, distance).wait_send()
        return carry

    lax.fori_loop(0, sp_count, finish, 0)
    lax.fori_loop(1, sp_count, finish_far, 0)
    lax.fori_loop(0, chunks, finish_back, 0)


def per_device(
    stream, mix_gain, pool_weight, pool_scale, ffn_gain, routes, route_weight, w_gate, w_up, w_down
):
    tok_rows, group_width = stream.shape
    tp_count = lax.axis_size("tp")
    sp_count = lax.axis_size("sp")
    width = group_width * tp_count
    tok_count, top_count = routes.shape
    cap = 2 * tok_count * top_count // sp_count
    halo_rows = 2 ** (pool_weight.shape[0] * tp_count)
    highs = tp_count // LANES
    chunks = chunk_count(sp_count)
    chunk_rows = sp_count // chunks * tp_count * cap
    ff_width = w_gate.shape[2]
    half = jnp.bfloat16
    vmem = pl.BlockSpec(memory_space=pltpu.VMEM)
    hbm = pl.BlockSpec(memory_space=pl.ANY)
    dma = pltpu.SemaphoreType.DMA
    rounds = max(1, sp_count // LANES - 1)
    return pl.pallas_call(
        functools.partial(expert_kernel, sp_count, tp_count, cap),
        out_shape=jax.ShapeDtypeStruct((tok_count, width), half),
        in_specs=[vmem] * 7 + [hbm] * 3,
        out_specs=vmem,
        scratch_shapes=[
            pltpu.VMEM((tp_count, 8, tok_rows), jnp.float32),
            pltpu.VMEM((tp_count, top_count, tok_count), jnp.int32),
            pltpu.VMEM((halo_rows, group_width), half),
            pltpu.VMEM((halo_rows, group_width), half),
            pltpu.VMEM((tp_count, tok_count, group_width), half),
            pltpu.VMEM((highs - 1, tp_count, tok_count, group_width), half),
            pltpu.VMEM((tp_count, tok_count, group_width), half),
            pltpu.VMEM((tp_count, top_count, sp_count * cap, tok_count), half),
            pltpu.VMEM((sp_count, LANES, highs, cap, group_width), half),
            pltpu.VMEM((highs - 1, min(NEAR, sp_count), LANES, highs, cap, group_width), half),
            pltpu.VMEM(w_gate.shape[1:], half),
            pltpu.VMEM(w_up.shape[1:], half),
            pltpu.VMEM(w_down.shape[1:], half),
            pltpu.VMEM((sp_count, LANES, highs, cap, width), half),
            pltpu.VMEM((chunk_rows, width), half),
            pltpu.VMEM((chunk_rows, ff_width), half),
            pltpu.VMEM((sp_count, LANES, highs, cap, width), half),
            pltpu.VMEM((sp_count, highs, cap, width), half),
            pltpu.VMEM((highs - 1, sp_count, cap, width), half),
            pltpu.VMEM((highs - 1, sp_count, cap, width), half),
            pltpu.VMEM((sp_count, cap, width), half),
            pltpu.VMEM((sp_count, cap, width), half),
            pltpu.VMEM((tok_count, width), jnp.float32),
            pltpu.SemaphoreType.REGULAR((rounds,)),
            dma((2, tp_count - 1)),
            dma((2, tp_count - 1)),
            dma((2,)),
            dma((2, highs - 1)),
            dma((2, highs)),
            dma((3,)),
            dma((sp_count,)),
            dma((sp_count,)),
            dma((min(NEAR, sp_count), highs - 1)),
            dma((sp_count, highs - 1)),
            dma((sp_count, highs - 1)),
            dma((sp_count, highs)),
            dma((sp_count, highs)),
            dma((2, chunks, HALVES)),
            dma((2, chunks, HALVES, highs - 1)),
            dma((sp_count, HALVES)),
            dma((sp_count, HALVES)),
        ],
        compiler_params=pltpu.CompilerParams(
            collective_id=1, has_side_effects=True, vmem_limit_bytes=60 * 1024 * 1024
        ),
    )(
        stream,
        mix_gain,
        pool_weight,
        pool_scale,
        ffn_gain,
        routes.T,
        route_weight.T,
        w_gate,
        w_up,
        w_down,
    )


def solution(mesh):
    in_specs = (
        P("sp", "tp"),
        P("tp"),
        P("tp", None, None),
        P("tp"),
        P(),
        P(("sp", "tp"), None),
        P(("sp", "tp"), None),
        P("sp", None, "tp"),
        P("sp", None, "tp"),
        P("sp", "tp", None),
    )
    out_specs = P(("sp", "tp"), None)
    return jax.shard_map(
        per_device, mesh=mesh, in_specs=in_specs, out_specs=out_specs, check_vma=False
    )
```
